32 devices in a mesh: sp: 8 (over z, x), tp: 4 (over y, core).
Axes of the slice: x: 2, y: 2, z: 4, core: 2. Of those that a mesh axis runs over, the one named last changes fastest.
Arguments:
- queries: bfloat16 [2048, 1024], P('sp', 'tp'), may hold values from -6 to 6
- keys: bfloat16 [2048, 1024], P('sp', 'tp'), may hold values from -72 to 72
- values: bfloat16 [2048, 1024], P('sp', 'tp'), may hold values from -6 to 6
- score_offset: float32 [8], P('tp'), may hold values from 2 to 11
- head_gain: float32 [128], replicated, may hold values from 0.1 to 1.9
- out_weight: bfloat16 [1024, 2048], P('tp'), may hold values from -0.1875 to 0.1875
- residual: bfloat16 [2048, 2048], P(('sp', 'tp')), may hold values from -6 to 6
- ln1_gain: float32 [2048], replicated, may hold values from 0.1 to 1.9
- ln1_bias: float32 [2048], replicated, may hold values from -2.5 to 2.5
- expert_ids: int32 [2048, 2], P(('sp', 'tp')), may hold values from 0 to 7, all different within a row; in each aligned block of 64 rows (0 to 63, 64 to 127, ...) at most 32 rows name the same one
- route_logits: float32 [2048, 2], P(('sp', 'tp')), may hold values from -6 to 6
- gate_weight: bfloat16 [8, 2048, 3072], P('sp', None, 'tp'), may hold values from -0.125 to 0.125
- up_weight: bfloat16 [8, 2048, 3072], P('sp', None, 'tp'), may hold values from -0.125 to 0.125
- down_weight: bfloat16 [8, 3072, 2048], P('sp', 'tp'), may hold values from -0.109375 to 0.109375
- ln2_gain: float32 [2048], replicated, may hold values from 0.1 to 1.9
- ln2_bias: float32 [2048], replicated, may hold values from -2.5 to 2.5
Outputs:
- output: bfloat16 [2048, 2048], P(('sp', 'tp'))
The draws below stay inside these ranges and needn't reach their ends.
Inputs may be any that keep to these rules, and one draw needn't show every extreme that they name: `expert_ids`: each row names 2 different experts. In the rows of one device no expert is named by more than 32 rows, and in every draw some expert is named by exactly 32 rows of some device.
All inputs are finite; a program needn't handle non-finite values.
Results may differ from the reference program's by a relative error of at most 0.012.
Values may be sent and summed in bfloat16 or wider, within the bound.
A program may use at most 128 MiB of HBM per device.

```python
import math
import jax
import jax.numpy as jnp
import numpy as np
from jax import lax

D = 2048
HEADS = 8
HD = 128
FF = 3072
TOP = 2
TOK_DEV = 256
SB_WIDTH = 1024
SEQUENCE_TOKENS = 2048
EXPERTS = 8
CAP = 32
N_SP = 8
N_TP = 4


def draw_keys(key, part):
    starting_key, key_for_block, spike_key = jax.random.split(key, 3)
    base = jnp.clip(jax.random.normal(starting_key, (SEQUENCE_TOKENS, SB_WIDTH), jnp.float32), -6.0, 6.0)
    low_scale = 0.6
    high_scale = 1.5
    blocks = jnp.exp(jax.random.uniform(key_for_block, (SEQUENCE_TOKENS // TOK_DEV,), jnp.float32, jnp.log(low_scale), jnp.log(high_scale)))
    row_scale = jnp.repeat(blocks, TOK_DEV)
    spike_position = jax.random.randint(spike_key, (8,), 0, SEQUENCE_TOKENS)
    spiking_flag = jnp.any(jnp.arange(SEQUENCE_TOKENS)[:, None] == spike_position[None, :], axis=1)
    row_scale = jnp.where(spiking_flag, 12.0, row_scale)
    return (base * row_scale[:, None]).astype(jnp.bfloat16)


def draw_score_offset(key, part):
    pick_key, fast_key, slow_key = jax.random.split(key, 3)
    slow_value = jax.random.uniform(slow_key, (HEADS,), jnp.float32, 9.5, 11.0)
    fast_value = jax.random.uniform(fast_key, (HEADS,), jnp.float32, 2.0, 4.0)
    slow_heads = jax.random.randint(pick_key, (HEADS,), 0, 2) == 1
    return jnp.where(slow_heads, slow_value, fast_value)


def block_levels(own_key, dims, pieces, least, top_value):
    loudness = 1.0
    for dim, parts in pieces:
        heights = jax.random.uniform(jax.random.fold_in(jax.random.fold_in(own_key, 6), dim), (parts,), jnp.float32, least / len(pieces), top_value / len(pieces))
        loudness = loudness * jnp.repeat(jnp.exp(heights), dims[dim] // parts).reshape((-1,) + (1,) * (len(dims) - 1 - dim))
    return loudness


def deal_out(key, own, number, rows, number_of, top, most, skew):
    order = jax.random.permutation(key, number_of)
    heavy_load, ordinary = portions_of(number_of, rows * top, most, skew, True), portions_of(number_of, rows * top, most, skew, False)
    places = jnp.arange(number_of)

    def named(tallies, rotation):
        used = int((tallies > 0).sum())
        fixed = max(1, used // 4)
        moved = fixed + (places - fixed + rotation * (used - fixed)) % max(1, number_of - fixed)
        return jnp.zeros((number_of,), jnp.int32).at[order[jnp.where(places < fixed, places, moved)]].set(jnp.asarray(tallies, jnp.int32))

    tallies = jnp.where(number % 4 == 0, named(heavy_load, number // 4), named(ordinary, number - number // 4 - 1))
    mixed = jax.random.permutation(jax.random.fold_in(own, 3), number_of)
    donor, receiver = mixed[0:number_of // 2 * 2:2], mixed[1:number_of // 2 * 2:2]
    room = jnp.minimum(tallies[donor] - 1, most - tallies[receiver]) // 2
    room = jnp.where((donor == order[0]) | (receiver == order[0]) | (tallies[receiver] == 0), 0, jnp.maximum(room, 0))
    moved = jax.random.randint(jax.random.fold_in(own, 4), (number_of // 2,), 0, 1 << 20) % (room + 1)
    tallies = tallies.at[donor].add(-moved).at[receiver].add(moved)
    members = jnp.searchsorted(jnp.cumsum(tallies), jnp.arange(rows * top), side="right").astype(jnp.int32)
    listing = members.reshape(top, rows).T
    listing = listing[jax.random.permutation(jax.random.fold_in(own, 1), rows)]
    rotation = jax.random.randint(jax.random.fold_in(own, 2), (rows, 1), 0, top)
    return jnp.take_along_axis(listing, (jnp.arange(top)[None, :] + rotation) % top, axis=1)


def portions_of(number_of, total, reach, lean, full):
    portions = [(1 << 20) // math.isqrt(grade ** lean) + 1 for grade in range(1, number_of + 1)]
    largest = reach if full else min(reach, max(-(-total // number_of), total * portions[0] // sum(portions)))
    least = 1 if total - largest >= number_of - 1 else 0
    given, rest = [largest] + [least] * (number_of - 1), total - largest - least * (number_of - 1)
    while rest > 0:
        free = [i for i in range(1, number_of) if given[i] < largest] or [i for i in range(1, number_of) if given[i] < reach]
        whole, remaining = sum([portions[i] for i in free]), rest
        for i in free:
            extra = min(reach - given[i], max(1, remaining * portions[i] // whole), rest)
            given[i] = given[i] + extra
            rest = rest - extra
    return np.array(given)


def bell_draw(rng, dims, spread, bound, shards=(), kind=jnp.bfloat16):
    level = block_levels(rng, dims, shards, -0.22, 0.18) if shards else 1.0
    array = jax.random.normal(rng, dims, jnp.float32) * spread * level
    return jnp.minimum(jnp.maximum(array, -bound), bound).astype(kind)


def setup_inputs(seed: int = 0) -> dict:
    seeds = jax.random.split(jax.random.key(seed), 17)
    queries = bell_draw(seeds[0], (SEQUENCE_TOKENS, SB_WIDTH), 1.0, 6.0, ((0, 8), (1, 4)))
    keys = draw_keys(jax.random.fold_in(seeds[16], 71), 0)
    values = bell_draw(seeds[2], (SEQUENCE_TOKENS, SB_WIDTH), 1.0, 6.0, ((0, 8), (1, 4)))
    score_offset = draw_score_offset(jax.random.fold_in(seeds[16], 71), 0)
    head_gain = jnp.clip(1.0 + 0.18 * jax.random.normal(seeds[4], (HD,), jnp.float32), 0.1, 1.9)
    out_weight = bell_draw(seeds[5], (SB_WIDTH, D), SB_WIDTH ** -0.5, 0.1875, ((0, 4),))
    residual = bell_draw(seeds[6], (SEQUENCE_TOKENS, D), 1.0, 6.0, ((0, 32),))
    ln1_gain = jnp.clip(1.0 + 0.18 * jax.random.normal(seeds[7], (D,), jnp.float32), 0.1, 1.9)
    ln1_bias = bell_draw(seeds[8], (D,), 0.3, 2.5, (), jnp.float32)
    expert_ids_keys = jax.random.split(jax.random.fold_in(seeds[9], 1), SEQUENCE_TOKENS // (TOK_DEV // N_TP))
    expert_ids_turns = jax.random.permutation(jax.random.fold_in(seeds[9], 3), SEQUENCE_TOKENS // (TOK_DEV // N_TP))
    expert_ids = jax.vmap(lambda own, number: deal_out(jax.random.fold_in(seeds[9], 2), own, number, TOK_DEV // N_TP, EXPERTS, TOP, CAP, 1))(expert_ids_keys, expert_ids_turns).reshape((SEQUENCE_TOKENS, TOP))
    route_logits = bell_draw(seeds[10], (SEQUENCE_TOKENS, TOP), 1.5, 6.0, ((0, 32),), jnp.float32)
    gate_weight = bell_draw(seeds[11], (EXPERTS, D, FF), D ** -0.5, 0.125, ((0, 8), (2, 4)))
    up_weight = bell_draw(seeds[12], (EXPERTS, D, FF), D ** -0.5, 0.125, ((0, 8), (2, 4)))
    down_weight = bell_draw(seeds[13], (EXPERTS, FF, D), FF ** -0.5, 0.109375, ((0, 8), (1, 4)))
    ln2_gain = jnp.clip(1.0 + 0.18 * jax.random.normal(seeds[14], (D,), jnp.float32), 0.1, 1.9)
    ln2_bias = bell_draw(seeds[15], (D,), 0.3, 2.5, (), jnp.float32)
    return {"queries": queries, "keys": keys, "values": values, "score_offset": score_offset, "head_gain": head_gain, "out_weight": out_weight, "residual": residual, "ln1_gain": ln1_gain, "ln1_bias": ln1_bias, "expert_ids": expert_ids, "route_logits": route_logits, "gate_weight": gate_weight, "up_weight": up_weight, "down_weight": down_weight, "ln2_gain": ln2_gain, "ln2_bias": ln2_bias}


residual_scale = 8.0 ** 0.25
norm_eps = 1e-05
head_eps = 1e-06

def layer_norm(inputs, gain, shift):
    mean_value = lax.optimization_barrier(jnp.mean(inputs, axis=-1, keepdims=True))
    centred = inputs - mean_value
    variance = lax.optimization_barrier(jnp.mean(centred * centred, axis=-1, keepdims=True))
    return centred * lax.rsqrt(variance + norm_eps) * gain + shift

def reference(queries, keys, values, score_offset, head_gain, out_weight, residual, ln1_gain, ln1_bias, expert_ids, route_logits, gate_weight, up_weight, down_weight, ln2_gain, ln2_bias):
    query_heads = queries.astype(jnp.float32).reshape(SEQUENCE_TOKENS, HEADS, HD)
    key_heads = keys.astype(jnp.float32).reshape(SEQUENCE_TOKENS, HEADS, HD)
    value_heads = values.astype(jnp.float32).reshape(SEQUENCE_TOKENS, HEADS, HD)
    block_rows = math.gcd(SEQUENCE_TOKENS, 256)
    key_pos = jnp.arange(SEQUENCE_TOKENS, dtype=jnp.int32)
    scale = HD ** (-0.5)

    def one_block(begin):
        block_queries = lax.dynamic_slice_in_dim(query_heads, begin, block_rows, 0)
        scores = jnp.einsum('qhd,khd->hqk', block_queries, key_heads) * scale - score_offset[:, None, None]
        query_pos = begin + jnp.arange(block_rows, dtype=jnp.int32)
        causal = (key_pos[None, :] < query_pos[:, None])[None]
        log_keep = jnp.where(causal, jax.nn.log_sigmoid(-scores), 0.0)
        tail_sum = lax.cumsum(log_keep, axis=2, reverse=True) - log_keep
        stick = jnp.where(causal, jnp.exp(jax.nn.log_sigmoid(scores) + tail_sum), 0.0)
        rounded = lax.optimization_barrier(stick.astype(jnp.bfloat16)).astype(jnp.float32)
        mixed = jnp.einsum('hqk,khd->qhd', rounded, value_heads)
        square_mean = lax.optimization_barrier(jnp.mean(mixed * mixed, axis=-1, keepdims=True))
        return (mixed * lax.rsqrt(square_mean + head_eps) * head_gain).astype(jnp.bfloat16)
    begins = jnp.arange(SEQUENCE_TOKENS // block_rows, dtype=jnp.int32) * block_rows
    att_out = lax.map(one_block, begins).reshape(SEQUENCE_TOKENS, SB_WIDTH)
    mixer = jnp.dot(att_out, out_weight, preferred_element_type=jnp.float32)
    hidden_in = layer_norm(residual_scale * residual.astype(jnp.float32) + mixer, ln1_gain, ln1_bias).astype(jnp.bfloat16)
    flat_ids = expert_ids.reshape(-1)
    limit = N_SP * N_TP * CAP
    hidden_units = FF // N_TP

    def per_expert(collected, expert):
        found = jnp.nonzero(flat_ids == expert, size=limit, fill_value=SEQUENCE_TOKENS * TOP)[0].astype(jnp.int32)
        token_rows = hidden_in[jnp.minimum(found // TOP, SEQUENCE_TOKENS - 1)]
        gate_part = jnp.dot(token_rows, gate_weight[expert], preferred_element_type=jnp.float32)
        up_part = jnp.dot(token_rows, up_weight[expert], preferred_element_type=jnp.float32)
        active = (jax.nn.silu(gate_part) * up_part).astype(jnp.bfloat16)
        summed = jnp.zeros((limit, D), jnp.float32)
        for index in range(N_TP):
            part = jnp.dot(active[:, index * hidden_units:(index + 1) * hidden_units], down_weight[expert, index * hidden_units:(index + 1) * hidden_units], preferred_element_type=jnp.float32)
            summed = summed + lax.optimization_barrier(part.astype(jnp.bfloat16)).astype(jnp.float32)
        collected = collected.at[found].set(summed.astype(jnp.bfloat16), mode='drop')
        return (collected, None)
    collected, _ = lax.scan(per_expert, jnp.zeros((SEQUENCE_TOKENS * TOP, D), jnp.bfloat16), jnp.arange(EXPERTS, dtype=jnp.int32))
    gates = jax.nn.softmax(route_logits.astype(jnp.float32), axis=-1)
    routed = lax.optimization_barrier(jnp.sum(gates[:, :, None] * collected.reshape(SEQUENCE_TOKENS, TOP, D).astype(jnp.float32), axis=1))
    return layer_norm(residual_scale * hidden_in.astype(jnp.float32) + routed, ln2_gain, ln2_bias).astype(jnp.bfloat16)
```

```python
import functools
import jax
import jax.numpy as jnp
from jax import lax
from jax.experimental import pallas as pl
from jax.experimental.pallas import tpu as pltpu
from jax.sharding import PartitionSpec as P

residual_scale = 8.0**0.25
norm_eps = 1e-05
head_eps = 1e-06


def layer_norm(inputs, gain, shift):
    mean_value = jnp.mean(inputs, axis=-1, keepdims=True)
    centred = inputs - mean_value
    variance = jnp.mean(centred * centred, axis=-1, keepdims=True)
    return centred * lax.rsqrt(variance + norm_eps) * gain + shift


def attend(query_rows, first_pos, key_rows, value_rows, score_offset, head_gain, key_span):
    query_count = query_rows.shape[0]
    heads = score_offset.shape[0]
    head_dim = query_rows.shape[1] // heads
    query_heads = query_rows.reshape(query_count, heads, head_dim)
    query_pos = first_pos + jnp.arange(query_count, dtype=jnp.int32)
    last_block = (first_pos + query_count - 1) // key_span
    scale = head_dim ** (-0.5)

    def turn(step, carry):
        totals, survive = carry
        block_index = last_block - step
        key_tile_block = lax.dynamic_slice_in_dim(
            key_rows, block_index * key_span, key_span, 0
        ).reshape(key_span, heads, head_dim)
        value_block = lax.dynamic_slice_in_dim(
            value_rows, block_index * key_span, key_span, 0
        ).reshape(key_span, heads, head_dim)
        scores = (
            jnp.einsum(
                "qhd,khd->hqk", query_heads, key_tile_block, preferred_element_type=jnp.float32
            )
            * scale
            - score_offset[:, None, None]
        )
        key_pos = block_index * key_span + jnp.arange(key_span, dtype=jnp.int32)
        causal = (key_pos[None, :] < query_pos[:, None])[None]
        log_keep = jnp.where(causal, jax.nn.log_sigmoid(-scores), 0.0)
        tail_sum = lax.cumsum(log_keep, axis=2, reverse=True) - log_keep
        weight_values = jnp.where(
            causal, jnp.exp(jax.nn.log_sigmoid(scores) + tail_sum + survive[:, :, None]), 0.0
        ).astype(jnp.bfloat16)
        totals = totals + jnp.einsum(
            "hqk,khd->qhd", weight_values, value_block, preferred_element_type=jnp.float32
        )
        return (totals, survive + jnp.sum(log_keep, axis=2))

    start_carry = (
        jnp.zeros((query_count, heads, head_dim), jnp.float32),
        jnp.zeros((heads, query_count), jnp.float32),
    )
    totals, _ = lax.fori_loop(0, last_block + 1, turn, start_carry)
    square_mean = jnp.mean(totals * totals, axis=-1, keepdims=True)
    normed = totals * lax.rsqrt(square_mean + head_eps) * head_gain
    return normed.reshape(query_count, heads * head_dim).astype(jnp.bfloat16)


def on_device(
    queries,
    keys,
    values,
    score_offset,
    head_gain,
    out_weight,
    residual,
    ln1_gain,
    ln1_bias,
    expert_ids,
    route_logits,
    gate_weight,
    up_weight,
    down_weight,
    ln2_gain,
    ln2_bias,
):
    sp_index = lax.axis_index("sp")
    tok_dev = queries.shape[0]
    gathered_keys, gathered_values = (
        lax.all_gather(keys, "sp", axis=0, tiled=True),
        lax.all_gather(values, "sp", axis=0, tiled=True),
    )
    key_span = gathered_keys.shape[0]
    while key_span > 1024 and key_span % 2 == 0:
        key_span = key_span // 2
    first_own = sp_index * tok_dev
    att_out = attend(
        queries, first_own, gathered_keys, gathered_values, score_offset, head_gain, key_span
    )
    row_count = residual.shape[0]
    model_width = residual.shape[1]
    token_heads = lax.all_to_all(att_out, "tp", split_axis=0, concat_axis=1, tiled=True)
    mixer = jnp.dot(
        token_heads,
        lax.all_gather(out_weight, "tp", axis=0, tiled=True),
        preferred_element_type=jnp.float32,
    )
    hidden_in = layer_norm(
        residual_scale * residual.astype(jnp.float32) + mixer, ln1_gain, ln1_bias
    ).astype(jnp.bfloat16)
    top_count = expert_ids.shape[1]
    experts = lax.axis_size("sp")
    capacity = max(2, 2 * top_count * row_count // experts)
    flat_ids = expert_ids.reshape(-1)
    onehot = (flat_ids[:, None] == jnp.arange(experts, dtype=jnp.int32)[None, :]).astype(jnp.int32)
    slot_index = jnp.sum(jnp.cumsum(onehot, axis=0) * onehot, axis=1) - 1
    destination = flat_ids * capacity + slot_index
    send_rows = jnp.repeat(hidden_in, top_count, axis=0)
    outgoing = (
        jnp.zeros((experts * capacity, model_width), jnp.bfloat16).at[destination].set(send_rows)
    )
    outgoing = outgoing.reshape(experts, capacity, model_width)
    row_block = lax.all_gather(
        lax.all_to_all(outgoing, "sp", split_axis=0, concat_axis=0, tiled=True),
        "tp",
        axis=0,
        tiled=True,
    )
    block_count = row_block.shape[0]
    flat_rows = row_block.reshape(-1, model_width)
    gate_part = jnp.dot(flat_rows, gate_weight[0], preferred_element_type=jnp.float32)
    up_part = jnp.dot(flat_rows, up_weight[0], preferred_element_type=jnp.float32)
    active = (jax.nn.silu(gate_part) * up_part).astype(jnp.bfloat16)
    down_part = jnp.dot(active, down_weight[0], preferred_element_type=jnp.float32).astype(
        jnp.bfloat16
    )
    partials = down_part.reshape(block_count, -1, model_width)
    summed = (
        lax.psum_scatter(partials, "tp", scatter_dimension=0, tiled=True)
        .astype(jnp.float32)
        .astype(jnp.bfloat16)
    )
    returned_rows = lax.all_to_all(summed, "sp", split_axis=0, concat_axis=0, tiled=True)
    picked = returned_rows.reshape(experts * capacity, model_width)[destination].reshape(
        row_count, top_count, model_width
    )
    gates = jax.nn.softmax(route_logits, axis=-1)
    routed = jnp.sum(gates[:, :, None] * picked.astype(jnp.float32), axis=1)
    return layer_norm(
        residual_scale * hidden_in.astype(jnp.float32) + routed, ln2_gain, ln2_bias
    ).astype(jnp.bfloat16)


MESH = pl.DeviceIdType.MESH
f32 = jnp.float32
bf16 = jnp.bfloat16


def remote(src, dst, send, recv, slot, device):
    return pltpu.make_async_remote_copy(
        src_ref=src,
        dst_ref=dst,
        send_sem=send.at[slot],
        recv_sem=recv.at[slot],
        device_id=device,
        device_id_type=MESH,
    )


def selection(ids, sp, capacity, experts):
    rows = ids.shape[1]
    slot = lax.broadcasted_iota(jnp.int32, (experts * capacity, rows), 0)
    expert = slot // capacity
    place = (slot % capacity).astype(f32)
    named = [(ids[k : k + 1, :] ^ sp) == expert for k in range(ids.shape[0])]
    either = functools.reduce(jnp.logical_or, named)
    before = (
        lax.broadcasted_iota(jnp.int32, (rows, rows), 0)
        < lax.broadcasted_iota(jnp.int32, (rows, rows), 1)
    )
    rank = jnp.dot(
        either.astype(f32).astype(bf16), before.astype(f32).astype(bf16), preferred_element_type=f32
    )
    fits = rank == place
    return [jnp.where(jnp.logical_and(one, fits), 1.0, 0.0) for one in named]


def plan_of(teams, gates_in, downs_in):
    def work(g, fill):
        units = [f"U{g}{n}" for n in range(gates_in)] + [f"D{g}{n}" for n in range(downs_in)]
        out, fill = [f"G{g}"], list(fill)
        for at, unit in enumerate(units):
            out.append(unit)
            out += fill[at * len(fill) // len(units) : (at + 1) * len(fill) // len(units)]
        return out

    plan = ["F0", "F1", "R0", "F2", "F3", "R1", "F6", "W"]
    plan += work(0, ["R2", "R3"]) + ["P0", "P1", "F7"]
    plan += work(1, ["R6", "F4"]) + ["P2", "P3", "R7"]
    plan += work(2, ["X2", "X3", "R4", "F5"]) + ["P6", "P7", "X6", "X7", "R5"]
    plan += work(3, ["N2", "N3", "N6", "N7"]) + ["P4", "P5", "X4", "X5"]
    plan += ["X1", "X0", "N4", "N5", "N1", "N0"]
    return plan


def layer_kernel(
    chain, experts, capacity, pieces,
    q_ref, k_ref, v_ref, off_ref, hgain_ref, ow_hbm, res_ref, g1_ref, b1_ref, ids_ref,
    log_ref, g2_ref, b2_ref, wg_hbm, wu_hbm, wd_hbm,
    y_ref,
    hid_ref, out_ref, kv, qb, acc, surv, tri, att, th, owf, mix,
    rows, wg, wu, wd, act, part, duo, ysend, yrecv, fin, ret,
    lsem, xs, xr, zs, zr, ps, pr, ws, wr,
    wsem, s0, r0, s1, r1, s2, r2, s3, r3, s4, r4, s5, r5, s6, r6,
):
    sp, tp = lax.axis_index("sp"), lax.axis_index("tp")
    z, x = sp // 2, sp % 2
    tok, hd = q_ref.shape[0], hgain_ref.shape[1]
    row_count = res_ref.shape[0]
    width = res_ref.shape[1]
    units = wg.shape[1]
    span = 2 * tok
    has_next = z + 1 < chain

    plane = [(m, (sp ^ (m & 1), tp ^ (m >> 1))) for m in range(1, 8)]
    barrier = pltpu.get_barrier_semaphore()
    others = [(sp ^ i, tp) for i in range(1, experts)]
    greeted = [device for _, device in plane] + others[1:]
    for device in greeted:
        pl.semaphore_signal(barrier, inc=1, device_id=device, device_id_type=MESH)
    mine = pl.ds(pl.multiple_of(x * tok, tok), tok)
    theirs = pl.ds(pl.multiple_of((1 - x) * tok, tok), tok)
    own_cols = pl.ds(pl.multiple_of(x * hd, hd), hd)
    peer_cols = pl.ds(pl.multiple_of((1 - x) * hd, hd), hd)
    local = [
        pltpu.make_async_copy(k_ref.at[:, own_cols], kv.at[0, 0, mine], lsem.at[0]),
        pltpu.make_async_copy(v_ref.at[:, own_cols], kv.at[0, 1, mine], lsem.at[1]),
        pltpu.make_async_copy(q_ref.at[:, own_cols], qb.at[mine], lsem.at[2]),
        pltpu.make_async_copy(ow_hbm, owf.at[0], lsem.at[3]),
    ]
    weights = [
        pltpu.make_async_copy(wg_hbm.at[0], wg, wsem.at[0]),
        pltpu.make_async_copy(wu_hbm.at[0], wu, wsem.at[1]),
        pltpu.make_async_copy(wd_hbm.at[0], wd, wsem.at[2]),
    ]
    for copy in local + weights:
        copy.start()
    pl.semaphore_wait(barrier, len(greeted))

    pair = (sp ^ 1, tp)
    swaps = [
        remote(k_ref.at[:, peer_cols], kv.at[0, 0, mine], xs, xr, 0, pair),
        remote(v_ref.at[:, peer_cols], kv.at[0, 1, mine], xs, xr, 1, pair),
        remote(q_ref.at[:, peer_cols], qb.at[mine], xs, xr, 2, pair),
    ]
    for copy in swaps:
        copy.start()
    across, beside = (sp, tp ^ 2), (sp, tp ^ 1)
    half = owf.shape[1] // 2
    strip = half // pieces

    def strip_of(side, p):
        return pl.ds(pl.multiple_of(side * half + p * strip, strip), strip)

    def weight_copy(src, dst, side, p, slot, device):
        at = strip_of(side, p)
        return remote(owf.at[src, at], owf.at[dst, at], ws, wr, slot, device)

    near = remote(owf.at[0], owf.at[1], ws, wr, 4 * pieces, beside)
    wide = [weight_copy(0, 2, x, p, p, across) for p in range(pieces)]
    side = [weight_copy(2, 2, x, p, pieces + p, pair) for p in range(pieces)]
    pass_own = [weight_copy(2, 3, x, p, 2 * pieces + p, beside) for p in range(pieces)]
    pass_far = [weight_copy(2, 3, 1 - x, p, 3 * pieces + p, beside) for p in range(pieces)]

    def weight_step(p):
        wide[p].wait_recv()
        side[p].start()
        pass_own[p].start()

    def hop(d, part, h):
        where = mine if h == 0 else theirs
        slot = (d * 2 + part) * 2 + h
        return pltpu.make_async_remote_copy(
            src_ref=kv.at[d, part, where],
            dst_ref=kv.at[d + 1, part, where],
            send_sem=zs.at[slot],
            recv_sem=zr.at[slot],
            device_id=(sp + 2, tp),
            device_id_type=MESH,
        )

    tri[...] = jnp.where(
        lax.broadcasted_iota(jnp.int32, tri.shape, 0)
        > lax.broadcasted_iota(jnp.int32, tri.shape, 1),
        -1.0,
        0.0,
    ).astype(bf16)
    acc[...] = jnp.zeros_like(acc)
    surv[...] = jnp.zeros_like(surv)
    log2e = 1.4426950408889634
    scale = hd ** (-0.5) * log2e
    offset = jnp.where(x == 0, off_ref[0], off_ref[1]) * log2e
    q_tile, k_tile = span, tri.shape[0]

    def block(d):
        for t in range(span // q_tile):
            at = pl.ds(t * q_tile, q_tile)
            query = qb[at, :]
            out, survive = acc[at, :], surv[at, :]
            for kb in reversed(range(span // k_tile)):
                if d == 0 and kb * k_tile >= (t + 1) * q_tile:
                    continue
                edge = d == 0 and (kb + 1) * k_tile > t * q_tile
                keys = kv[d, 0, pl.ds(kb * k_tile, k_tile), :]
                scores = (
                    lax.dot_general(
                        query, keys, (((1,), (1,)), ((), ())), preferred_element_type=f32
                    )
                    * scale
                    - offset
                )
                drop = jnp.maximum(scores, 0.0) + log2e * jnp.log(1.0 + jnp.exp2(-jnp.abs(scores)))
                take = scores - drop
                if edge:
                    causal = (
                        lax.broadcasted_iota(jnp.int32, (q_tile, k_tile), 1) + kb * k_tile
                        < lax.broadcasted_iota(jnp.int32, (q_tile, k_tile), 0) + t * q_tile
                    )
                    drop = jnp.where(causal, drop, 0.0)
                top = drop.astype(bf16)
                low = (drop - top.astype(f32)).astype(bf16)
                tail = jnp.dot(top, tri[...], preferred_element_type=f32) + jnp.dot(
                    low, tri[...], preferred_element_type=f32
                )
                weight = jnp.exp2(take + tail + survive)
                if edge:
                    weight = jnp.where(causal, weight, 0.0)
                out = out + jnp.dot(
                    weight.astype(bf16),
                    kv[d, 1, pl.ds(kb * k_tile, k_tile), :],
                    preferred_element_type=f32,
                )
                survive = survive + (tail[:, :1] - drop[:, :1])
            acc[at, :] = out
            surv[at, :] = survive

    local[0].wait()
    local[1].wait()

    @pl.when(has_next)
    def _():
        hop(0, 0, 0).start()
        hop(0, 1, 0).start()

    local[3].wait()
    for copy in wide:
        copy.start()
    near.start()

    def receive(d, h):
        for part in range(2):
            hop(d - 1, part, h).wait_recv()
            if d + 1 < chain:

                @pl.when(has_next)
                def _():
                    hop(d, part, h).start()

    @pl.when(z >= 1)
    def _():
        receive(1, 0)

    swaps[0].wait_recv()
    swaps[1].wait_recv()

    @pl.when(has_next)
    def _():
        hop(0, 0, 1).start()
        hop(0, 1, 1).start()

    local[2].wait()
    swaps[2].wait_recv()
    weight_step(0)
    block(0)
    weight_step(1)
    for d in range(1, chain):

        @pl.when(d <= z)
        def _(d=d):
            if d > 1:
                receive(d, 0)
            receive(d, 1)
            block(d)

        if d == 1:
            for p in range(2, pieces):
                weight_step(p)
    for p in range(pieces):
        side[p].wait_recv()
        pass_far[p].start()

    total = acc[...]
    normed = total * lax.rsqrt(jnp.mean(total * total, axis=1, keepdims=True) + head_eps)
    att[...] = (normed * hgain_ref[...]).astype(bf16)

    def block_of(m):
        start = (x ^ (m & 1)) * tok + (tp ^ (m >> 1)) * row_count
        return att.at[pl.ds(pl.multiple_of(start, row_count), row_count)]

    spread = [
        remote(block_of(m), th.at[m >> 1, x], ps, pr, m, device) for m, device in plane
    ]
    for copy in spread:
        copy.start()
    own = pltpu.make_async_copy(block_of(0), th.at[0, x], lsem.at[4])
    own.start()
    near.wait_recv()
    for copy in pass_own + pass_far:
        copy.wait_recv()
    own.wait()
    for copy in spread:
        copy.wait_recv()

    lefts = [jnp.concatenate([th[j, 0], th[j, 1]], axis=1) for j in range(4)]
    col = min(512, width)
    for n in range(width // col):
        cut = pl.ds(n * col, col)
        mix[:, cut] = functools.reduce(
            jnp.add,
            [jnp.dot(lefts[j], owf[j, :, cut], preferred_element_type=f32) for j in range(4)],
        )
    hidden = layer_norm(
        residual_scale * res_ref[...].astype(f32) + mix[...], g1_ref[...], b1_ref[...]
    ).astype(bf16)
    hid_ref[...] = hidden
    chosen = selection(ids_ref[...], sp, capacity, experts)
    pick = functools.reduce(jnp.add, chosen).astype(bf16)
    for n in range(width // col):
        cut = pl.ds(n * col, col)
        out_ref[:, :, cut] = (
            jnp.dot(pick, hidden[:, n * col : (n + 1) * col], preferred_element_type=f32)
            .astype(bf16)
            .reshape(experts, capacity, col)
        )
    own = pltpu.make_async_copy(out_ref.at[0], rows.at[0, 0], wsem.at[3])
    own.start()

    send = [None] + [
        remote(out_ref.at[i], rows.at[i, 0], s0, r0, i, others[i - 1]) for i in range(1, experts)
    ]
    to_y = [remote(rows.at[i, 0], rows.at[i, 2], s1, r1, i, across) for i in range(experts)]
    to_core = [remote(rows.at[i, 0], rows.at[i, 1], s2, r2, i, beside) for i in range(experts)]
    relay = [remote(rows.at[i, 2], rows.at[i, 3], s3, r3, i, beside) for i in range(experts)]
    pairs = [
        [remote(part.at[i, 1 + 2 * p], duo.at[i, p], s4, r4, 2 * i + p, beside) for p in range(2)]
        for i in range(experts)
    ]
    sums = [remote(ysend.at[i], yrecv.at[i], s5, r5, i, across) for i in range(experts)]
    back = [None] + [
        remote(fin.at[i], ret.at[i], s6, r6, i, others[i - 1]) for i in range(1, experts)
    ]
    near_self, near_z = (0, 1), (2, 3)
    far_three, far_two = tuple(range(6, experts)), tuple(range(4, min(6, experts)))
    teams = [team for team in (near_self, near_z, far_three, far_two) if team]
    for i in (1,) + near_z + far_three + far_two:
        send[i].start()
    tile = min(256, units)
    gates_in, downs_in = units // tile, width // col

    def enter(i):
        (own.wait if i == 0 else send[i].wait_recv)()
        to_y[i].start()
        to_core[i].start()

    def onward(i):
        to_y[i].wait_recv()
        relay[i].start()

    def gather(g):
        for i in teams[g]:
            to_core[i].wait_recv()
            relay[i].wait_recv()

    def hidden_units(g, n):
        team = teams[g]
        cut = pl.ds(n * tile, tile)
        given = rows[team[0] : team[0] + len(team)].reshape(-1, width)
        gate = jnp.dot(given, wg[:, cut], preferred_element_type=f32)
        up = jnp.dot(given, wu[:, cut], preferred_element_type=f32)
        act[:, cut] = (gate / (1.0 + jnp.exp(-gate)) * up).astype(bf16)

    def back_down(g, n):
        team = teams[g]
        cut = pl.ds(n * col, col)
        down = jnp.dot(act[...], wd[:, cut], preferred_element_type=f32).astype(bf16)
        part[team[0] : team[0] + len(team), :, :, cut] = down.reshape(len(team), 4, capacity, col)

    def pair_up(i):
        for p in (1, 0):
            pairs[i][p].start()

    def cross(i):
        pairs[i][1].wait_recv()
        ysend[i] = (part[i, 2].astype(f32) + duo[i, 1].astype(f32)).astype(bf16)
        sums[i].start()

    def finish(i):
        pairs[i][0].wait_recv()
        sums[i].wait_recv()
        total = part[i, 0].astype(f32) + duo[i, 0].astype(f32) + yrecv[i].astype(f32)
        if i == 0:
            ret[0] = total.astype(bf16)
        else:
            fin[i] = total.astype(bf16)
            back[i].start()

    def weights_in():
        for copy in weights:
            copy.wait()

    acts = {
        "F": enter, "R": onward, "G": gather, "P": pair_up, "X": cross, "N": finish,
        "U": hidden_units, "D": back_down, "W": weights_in,
    }

    def run(token):
        acts[token[0]](*[int(v) for v in token[1:]])

    for number, token in enumerate(plan_of(len(teams), gates_in, downs_in)):
        run(token)

    logits = log_ref[...]
    high = jnp.max(logits, axis=0, keepdims=True)
    grown = jnp.exp(logits - high)
    gates = grown / jnp.sum(grown, axis=0, keepdims=True)
    mixing = functools.reduce(
        jnp.add, [one * gates[k : k + 1, :] for k, one in enumerate(chosen)]
    ).T
    mix_top = mixing.astype(bf16)
    mix_low = (mixing - mix_top.astype(f32)).astype(bf16)
    for i in range(1, experts):
        back[i].wait_recv()
    slots = experts * capacity
    for n in range(width // col):
        cut = pl.ds(n * col, col)
        given = ret[:, :, cut].reshape(slots, col)
        mix[:, cut] = jnp.dot(mix_top, given, preferred_element_type=f32) + jnp.dot(
            mix_low, given, preferred_element_type=f32
        )
    y_ref[...] = layer_norm(
        residual_scale * hid_ref[...].astype(f32) + mix[...], g2_ref[...], b2_ref[...]
    ).astype(bf16)
    for copy in send[1:] + to_y + to_core + relay + sums + back[1:]:
        copy.wait_send()
    for two in pairs:
        for copy in two:
            copy.wait_send()
    for copy in swaps + wide + side + [near] + pass_own + pass_far + spread:
        copy.wait_send()
    for d in range(chain - 1):

        @pl.when(jnp.logical_and(d <= z, has_next))
        def _(d=d):
            for h in range(2):
                for part in range(2):
                    hop(d, part, h).wait_send()


def fused(
    queries, keys, values, score_offset, head_gain, out_weight, residual, ln1_gain, ln1_bias,
    expert_ids, route_logits, gate_weight, up_weight, down_weight, ln2_gain, ln2_bias,
):
    experts = lax.axis_size("sp")
    tok, hd = queries.shape[0], head_gain.shape[0]
    row_count, width = residual.shape
    capacity = max(2, 2 * expert_ids.shape[1] * row_count // experts)
    chain = experts // 2
    span = 2 * tok
    pieces = 4
    units = gate_weight.shape[2]
    vm = pl.BlockSpec(memory_space=pltpu.VMEM)
    sm = pl.BlockSpec(memory_space=pltpu.SMEM)
    hbm = pl.BlockSpec(memory_space=pl.ANY)
    dma = lambda n: pltpu.SemaphoreType.DMA((n,))
    limit = 62 * 1024 * 1024
    block = lambda *lead: pltpu.VMEM((*lead, capacity, width), bf16)
    n = experts
    return pl.pallas_call(
        functools.partial(layer_kernel, chain, experts, capacity, pieces),
        out_shape=jax.ShapeDtypeStruct((row_count, width), bf16),
        in_specs=[vm, vm, vm, sm, vm, hbm, vm, vm, vm, vm, vm, vm, vm, hbm, hbm, hbm],
        out_specs=vm,
        scratch_shapes=[
            pltpu.VMEM((row_count, width), bf16),
            block(n),
            pltpu.VMEM((chain, 2, span, hd), bf16),
            pltpu.VMEM((span, hd), bf16),
            pltpu.VMEM((span, hd), f32),
            pltpu.VMEM((span, 1), f32),
            pltpu.VMEM((min(256, tok), min(256, tok)), bf16),
            pltpu.VMEM((span, hd), bf16),
            pltpu.VMEM((4, 2, row_count, hd), bf16),
            pltpu.VMEM((4, out_weight.shape[0], width), bf16),
            pltpu.VMEM((row_count, width), f32),
            block(n, 4),
            pltpu.VMEM((width, units), bf16),
            pltpu.VMEM((width, units), bf16),
            pltpu.VMEM((units, width), bf16),
            pltpu.VMEM((8 * capacity, units), bf16),
            block(n, 4), block(n, 2), block(n), block(n), block(n), block(n),
            dma(5), dma(3), dma(3), dma(4 * chain), dma(4 * chain), dma(8), dma(8), dma(4 * pieces + 1),
            dma(4 * pieces + 1),
            dma(4),
            dma(n), dma(n), dma(n), dma(n), dma(n), dma(n), dma(n), dma(n),
            dma(2 * n), dma(2 * n), dma(n), dma(n), dma(n), dma(n),
        ],
        compiler_params=pltpu.CompilerParams(
            collective_id=0, has_side_effects=True, vmem_limit_bytes=limit
        ),
    )(
        queries, keys, values, score_offset, head_gain[None], out_weight, residual,
        ln1_gain[None], ln1_bias[None], expert_ids.T, route_logits.T,
        ln2_gain[None], ln2_bias[None], gate_weight, up_weight, down_weight,
    )


def program_for(*args):
    queries, head_gain, residual, ids = args[0], args[4], args[6], args[9]
    experts = lax.axis_size("sp")
    capacity = max(2, 2 * ids.shape[1] * residual.shape[0] // experts)
    rows_ok = capacity % 16 == 0 and residual.shape[0] % 16 == 0
    heads_ok = queries.shape[1] == 2 * head_gain.shape[0] and head_gain.shape[0] % 128 == 0
    mesh_ok = lax.axis_size("tp") == 4 and experts == 8
    whole = queries.shape[0] % 128 == 0 and args[11].shape[0] == 1
    if rows_ok and heads_ok and mesh_ok and whole:
        return fused(*args)
    return on_device(*args)


def solution(mesh):
    in_specs = (
        P("sp", "tp"),
        P("sp", "tp"),
        P("sp", "tp"),
        P("tp"),
        P(),
        P("tp", None),
        P(("sp", "tp"), None),
        P(),
        P(),
        P(("sp", "tp"), None),
        P(("sp", "tp"), None),
        P("sp", None, "tp"),
        P("sp", None, "tp"),
        P("sp", "tp", None),
        P(),
        P(),
    )
    out_specs = P(("sp", "tp"), None)
    return jax.shard_map(
        program_for, mesh=mesh, in_specs=in_specs, out_specs=out_specs, check_vma=False
    )
```

```python
import functools
import jax
import jax.numpy as jnp
from jax import lax
from jax.experimental import pallas as pl
from jax.experimental.pallas import tpu as pltpu
from jax.sharding import PartitionSpec as P

residual_scale = 8.0**0.25
norm_eps = 1e-05
head_eps = 1e-06


def layer_norm(inputs, gain, shift):
    mean_value = jnp.mean(inputs, axis=-1, keepdims=True)
    centred = inputs - mean_value
    variance = jnp.mean(centred * centred, axis=-1, keepdims=True)
    return centred * lax.rsqrt(variance + norm_eps) * gain + shift


def attend(query_rows, first_pos, key_rows, value_rows, score_offset, head_gain, key_span):
    query_count = query_rows.shape[0]
    heads = score_offset.shape[0]
    head_dim = query_rows.shape[1] // heads
    query_heads = query_rows.reshape(query_count, heads, head_dim)
    query_pos = first_pos + jnp.arange(query_count, dtype=jnp.int32)
    last_block = (first_pos + query_count - 1) // key_span
    scale = head_dim ** (-0.5)

    def turn(step, carry):
        totals, survive = carry
        block_index = last_block - step
        key_tile_block = lax.dynamic_slice_in_dim(
            key_rows, block_index * key_span, key_span, 0
        ).reshape(key_span, heads, head_dim)
        value_block = lax.dynamic_slice_in_dim(
            value_rows, block_index * key_span, key_span, 0
        ).reshape(key_span, heads, head_dim)
        scores = (
            jnp.einsum(
                "qhd,khd->hqk", query_heads, key_tile_block, preferred_element_type=jnp.float32
            )
            * scale
            - score_offset[:, None, None]
        )
        key_pos = block_index * key_span + jnp.arange(key_span, dtype=jnp.int32)
        causal = (key_pos[None, :] < query_pos[:, None])[None]
        log_keep = jnp.where(causal, jax.nn.log_sigmoid(-scores), 0.0)
        tail_sum = lax.cumsum(log_keep, axis=2, reverse=True) - log_keep
        weight_values = jnp.where(
            causal, jnp.exp(jax.nn.log_sigmoid(scores) + tail_sum + survive[:, :, None]), 0.0
        ).astype(jnp.bfloat16)
        totals = totals + jnp.einsum(
            "hqk,khd->qhd", weight_values, value_block, preferred_element_type=jnp.float32
        )
        return (totals, survive + jnp.sum(log_keep, axis=2))

    start_carry = (
        jnp.zeros((query_count, heads, head_dim), jnp.float32),
        jnp.zeros((heads, query_count), jnp.float32),
    )
    totals, _ = lax.fori_loop(0, last_block + 1, turn, start_carry)
    square_mean = jnp.mean(totals * totals, axis=-1, keepdims=True)
    normed = totals * lax.rsqrt(square_mean + head_eps) * head_gain
    return normed.reshape(query_count, heads * head_dim).astype(jnp.bfloat16)


def on_device(
    queries,
    keys,
    values,
    score_offset,
    head_gain,
    out_weight,
    residual,
    ln1_gain,
    ln1_bias,
    expert_ids,
    route_logits,
    gate_weight,
    up_weight,
    down_weight,
    ln2_gain,
    ln2_bias,
):
    sp_index = lax.axis_index("sp")
    tok_dev = queries.shape[0]
    gathered_keys, gathered_values = (
        lax.all_gather(keys, "sp", axis=0, tiled=True),
        lax.all_gather(values, "sp", axis=0, tiled=True),
    )
    key_span = gathered_keys.shape[0]
    while key_span > 1024 and key_span % 2 == 0:
        key_span = key_span // 2
    first_own = sp_index * tok_dev
    att_out = attend(
        queries, first_own, gathered_keys, gathered_values, score_offset, head_gain, key_span
    )
    row_count = residual.shape[0]
    model_width = residual.shape[1]
    token_heads = lax.all_to_all(att_out, "tp", split_axis=0, concat_axis=1, tiled=True)
    mixer = jnp.dot(
        token_heads,
        lax.all_gather(out_weight, "tp", axis=0, tiled=True),
        preferred_element_type=jnp.float32,
    )
    hidden_in = layer_norm(
        residual_scale * residual.astype(jnp.float32) + mixer, ln1_gain, ln1_bias
    ).astype(jnp.bfloat16)
    top_count = expert_ids.shape[1]
    experts = lax.axis_size("sp")
    capacity = max(2, 2 * top_count * row_count // experts)
    flat_ids = expert_ids.reshape(-1)
    onehot = (flat_ids[:, None] == jnp.arange(experts, dtype=jnp.int32)[None, :]).astype(jnp.int32)
    slot_index = jnp.sum(jnp.cumsum(onehot, axis=0) * onehot, axis=1) - 1
    destination = flat_ids * capacity + slot_index
    send_rows = jnp.repeat(hidden_in, top_count, axis=0)
    outgoing = (
        jnp.zeros((experts * capacity, model_width), jnp.bfloat16).at[destination].set(send_rows)
    )
    outgoing = outgoing.reshape(experts, capacity, model_width)
    row_block = lax.all_gather(
        lax.all_to_all(outgoing, "sp", split_axis=0, concat_axis=0, tiled=True),
        "tp",
        axis=0,
        tiled=True,
    )
    block_count = row_block.shape[0]
    flat_rows = row_block.reshape(-1, model_width)
    gate_part = jnp.dot(flat_rows, gate_weight[0], preferred_element_type=jnp.float32)
    up_part = jnp.dot(flat_rows, up_weight[0], preferred_element_type=jnp.float32)
    active = (jax.nn.silu(gate_part) * up_part).astype(jnp.bfloat16)
    down_part = jnp.dot(active, down_weight[0], preferred_element_type=jnp.float32).astype(
        jnp.bfloat16
    )
    partials = down_part.reshape(block_count, -1, model_width)
    summed = (
        lax.psum_scatter(partials, "tp", scatter_dimension=0, tiled=True)
        .astype(jnp.float32)
        .astype(jnp.bfloat16)
    )
    returned_rows = lax.all_to_all(summed, "sp", split_axis=0, concat_axis=0, tiled=True)
    picked = returned_rows.reshape(experts * capacity, model_width)[destination].reshape(
        row_count, top_count, model_width
    )
    gates = jax.nn.softmax(route_logits, axis=-1)
    routed = jnp.sum(gates[:, :, None] * picked.astype(jnp.float32), axis=1)
    return layer_norm(
        residual_scale * hidden_in.astype(jnp.float32) + routed, ln2_gain, ln2_bias
    ).astype(jnp.bfloat16)


MESH = pl.DeviceIdType.MESH
f32 = jnp.float32
bf16 = jnp.bfloat16


def remote(src, dst, send, recv, slot, device):
    return pltpu.make_async_remote_copy(
        src_ref=src,
        dst_ref=dst,
        send_sem=send.at[slot],
        recv_sem=recv.at[slot],
        device_id=device,
        device_id_type=MESH,
    )


def selection(ids, sp, capacity, experts):
    rows = ids.shape[1]
    slot = lax.broadcasted_iota(jnp.int32, (experts * capacity, rows), 0)
    expert = slot // capacity
    place = (slot % capacity).astype(f32)
    named = [(ids[k : k + 1, :] ^ sp) == expert for k in range(ids.shape[0])]
    either = functools.reduce(jnp.logical_or, named)
    before = (
        lax.broadcasted_iota(jnp.int32, (rows, rows), 0)
        < lax.broadcasted_iota(jnp.int32, (rows, rows), 1)
    )
    rank = jnp.dot(
        either.astype(f32).astype(bf16), before.astype(f32).astype(bf16), preferred_element_type=f32
    )
    fits = rank == place
    return [jnp.where(jnp.logical_and(one, fits), 1.0, 0.0) for one in named]


def plan_of(gates_in, downs_in):
    def work(g, fill):
        units = [f"U{g}{n}" for n in range(gates_in)] + [f"D{g}{n}" for n in range(downs_in)]
        out, fill = [f"G{g}"], list(fill)
        for at, unit in enumerate(units):
            out.append(unit)
            out += fill[at * len(fill) // len(units) : (at + 1) * len(fill) // len(units)]
        return out

    plan = ["S1", "S2", "S3", "S6", "S7", "S4", "S5", "F0", "F2", "F1", "R2", "F3", "W"]
    plan += work(0, ["F4", "R3"]) + ["P0", "P1", "N0", "N1", "F5"]
    plan += work(1, ["R4", "F6"]) + ["P2", "P3", "R5", "N2", "N3"]
    plan += work(2, ["F7", "R6"]) + ["P4", "P5", "X4", "X5", "R7"]
    plan += work(3, ["N4", "N5"]) + ["P6", "P7", "X6", "X7", "K", "N6", "N7", "L"]
    return plan


def layer_kernel(
    chain, experts, capacity, pieces, dup,
    q_hbm, k_hbm, v_hbm, off_hbm, hgain_hbm, ow_hbm, res_hbm, g1_hbm, b1_hbm, ids_hbm,
    log_hbm, g2_hbm, b2_hbm, wg_hbm, wu_hbm, wd_hbm,
    y_hbm,
    off_ref, hgain_ref, g1_ref, b1_ref, g2_ref, b2_ref, ids_ref, log_ref, res_ref, give, y_ref,
    hid_ref, out_ref, kv, qb, acc, surv, tri, att, th, owf, mix,
    rows, wg, wu, wd, act, part, duo, ysend, yrecv, fin, fin_far, ret, ret_far, csend, crecv,
    lsem, xs, xr, zs, zr, ps, pr, ws, wr,
    wsem, s0, r0, s1, r1, s2, r2, s3, r3, s4, r4, s5, r5, s6, r6, es, er, cs, cr,
):
    sp, tp = lax.axis_index("sp"), lax.axis_index("tp")
    z, x = sp // 2, sp % 2
    yy, core = tp // 2, tp % 2
    tok, hd = q_hbm.shape[0], hgain_ref.shape[1]
    row_count, width = res_hbm.shape
    units = wg.shape[1]
    span = 2 * tok
    has_next = z + 1 < chain
    half_dup = experts // 2

    plane = [(m, (sp ^ (m & 1), tp ^ (m >> 1))) for m in range(1, 8)]
    barrier = pltpu.get_barrier_semaphore()
    others = [(sp ^ i, tp) for i in range(1, experts)]
    greeted = [device for _, device in plane] + others[1:]
    for device in greeted:
        pl.semaphore_signal(barrier, inc=1, device_id=device, device_id_type=MESH)
    mine = pl.ds(pl.multiple_of(x * tok, tok), tok)
    theirs = pl.ds(pl.multiple_of((1 - x) * tok, tok), tok)
    own_cols = pl.ds(pl.multiple_of(x * hd, hd), hd)
    peer_cols = pl.ds(pl.multiple_of((1 - x) * hd, hd), hd)
    fetches = [
        (k_hbm.at[:, peer_cols], give.at[0]),
        (v_hbm.at[:, peer_cols], give.at[1]),
        (k_hbm.at[:, own_cols], kv.at[0, 0, mine]),
        (v_hbm.at[:, own_cols], kv.at[0, 1, mine]),
        (q_hbm.at[:, peer_cols], give.at[2]),
        (ow_hbm, owf.at[0]),
        (q_hbm.at[:, own_cols], qb.at[mine]),
        (ids_hbm, ids_ref.at[yy]),
        (log_hbm, log_ref.at[yy]),
        (res_hbm, res_ref.at[yy]),
        (off_hbm, off_ref),
        (hgain_hbm, hgain_ref),
        (g1_hbm, g1_ref),
        (b1_hbm, b1_ref),
        (g2_hbm, g2_ref),
        (b2_hbm, b2_ref),
    ]
    local = [
        pltpu.make_async_copy(src, dst, lsem.at[n]) for n, (src, dst) in enumerate(fetches)
    ]
    weights = [
        pltpu.make_async_copy(wg_hbm.at[0], wg, wsem.at[0]),
        pltpu.make_async_copy(wu_hbm.at[0], wu, wsem.at[1]),
        pltpu.make_async_copy(wd_hbm.at[0], wd, wsem.at[2]),
    ]
    for copy in local + weights:
        copy.start()

    tri[...] = jnp.where(
        lax.broadcasted_iota(jnp.int32, tri.shape, 0)
        > lax.broadcasted_iota(jnp.int32, tri.shape, 1),
        -1.0,
        0.0,
    ).astype(bf16)
    acc[...] = jnp.zeros_like(acc)
    surv[...] = jnp.zeros_like(surv)
    pl.semaphore_wait(barrier, len(greeted))

    pair = (sp ^ 1, tp)
    swaps = [
        remote(give.at[0], kv.at[0, 0, mine], xs, xr, 0, pair),
        remote(give.at[1], kv.at[0, 1, mine], xs, xr, 1, pair),
        remote(give.at[2], qb.at[mine], xs, xr, 2, pair),
    ]
    for n, at in enumerate((0, 1)):
        local[at].wait()
        swaps[n].start()
    across, beside = (sp, tp ^ 2), (sp, tp ^ 1)
    half = owf.shape[1] // 2
    strip = half // pieces

    def strip_of(side, p):
        return pl.ds(pl.multiple_of(side * half + p * strip, strip), strip)

    def weight_copy(src, dst, side, p, slot, device):
        at = strip_of(side, p)
        return remote(owf.at[src, at], owf.at[dst, at], ws, wr, slot, device)

    near = remote(owf.at[0], owf.at[1], ws, wr, 4 * pieces, beside)
    wide = [weight_copy(0, 2, x, p, p, across) for p in range(pieces)]
    side = [weight_copy(2, 2, x, p, pieces + p, pair) for p in range(pieces)]
    pass_own = [weight_copy(2, 3, x, p, 2 * pieces + p, beside) for p in range(pieces)]
    pass_far = [weight_copy(2, 3, 1 - x, p, 3 * pieces + p, beside) for p in range(pieces)]
    twins = [
        remote(ids_ref.at[yy], ids_ref.at[yy], es, er, 0, across),
        remote(log_ref.at[yy], log_ref.at[yy], es, er, 1, across),
        remote(res_ref.at[yy], res_ref.at[yy], es, er, 2, across),
    ]

    def weight_step(p):
        wide[p].wait_recv()
        side[p].start()
        pass_own[p].start()

    def hop(d, part, h):
        where = mine if h == 0 else theirs
        slot = (d * 2 + part) * 2 + h
        return pltpu.make_async_remote_copy(
            src_ref=kv.at[d, part, where],
            dst_ref=kv.at[d + 1, part, where],
            send_sem=zs.at[slot],
            recv_sem=zr.at[slot],
            device_id=(sp + 2, tp),
            device_id_type=MESH,
        )

    log2e = 1.4426950408889634
    scale = hd ** (-0.5) * log2e
    k_tile = tri.shape[0]

    def block(d):
        offset = jnp.where(x == 0, off_ref[0], off_ref[1]) * log2e
        for kb in reversed(range(span // k_tile)):
            lead = kb * k_tile if d == 0 else 0
            at = pl.ds(lead, span - lead)
            query = qb[at, :]
            out, survive = acc[at, :], surv[at, :]
            keys = kv[d, 0, pl.ds(kb * k_tile, k_tile), :]
            scores = (
                lax.dot_general(
                    query, keys, (((1,), (1,)), ((), ())), preferred_element_type=f32
                )
                * scale
                - offset
            )
            drop = jnp.maximum(scores, 0.0) + log2e * jnp.log(1.0 + jnp.exp2(-jnp.abs(scores)))
            take = scores - drop
            if d == 0:
                causal = (
                    lax.broadcasted_iota(jnp.int32, scores.shape, 1)
                    < lax.broadcasted_iota(jnp.int32, scores.shape, 0)
                )
                drop = jnp.where(causal, drop, 0.0)
            top = drop.astype(bf16)
            low = (drop - top.astype(f32)).astype(bf16)
            tail = jnp.dot(top, tri[...], preferred_element_type=f32) + jnp.dot(
                low, tri[...], preferred_element_type=f32
            )
            weight = jnp.exp2(take + tail + survive)
            if d == 0:
                weight = jnp.where(causal, weight, 0.0)
            acc[at, :] = out + jnp.dot(
                weight.astype(bf16),
                kv[d, 1, pl.ds(kb * k_tile, k_tile), :],
                preferred_element_type=f32,
            )
            surv[at, :] = survive + (tail[:, :1] - drop[:, :1])

    local[2].wait()
    local[3].wait()

    @pl.when(has_next)
    def _():
        hop(0, 0, 0).start()
        hop(0, 1, 0).start()

    local[4].wait()
    swaps[2].start()
    local[7].wait()
    twins[0].start()
    local[8].wait()
    twins[1].start()
    local[5].wait()
    for copy in wide:
        copy.start()
    local[9].wait()
    twins[2].start()
    near.start()

    def receive(d, h):
        for part in range(2):
            hop(d - 1, part, h).wait_recv()
            if d + 1 < chain:

                @pl.when(has_next)
                def _():
                    hop(d, part, h).start()

    @pl.when(z >= 1)
    def _():
        receive(1, 0)

    swaps[0].wait_recv()
    swaps[1].wait_recv()

    @pl.when(has_next)
    def _():
        hop(0, 0, 1).start()
        hop(0, 1, 1).start()

    for at in (6, 10, 11, 12, 13, 14, 15):
        local[at].wait()
    swaps[2].wait_recv()
    weight_step(0)
    block(0)
    weight_step(1)
    for d in range(1, chain):

        @pl.when(d <= z)
        def _(d=d):
            if d > 1:
                receive(d, 0)
            receive(d, 1)
            block(d)

        if d == 1:
            for p in range(2, pieces):
                weight_step(p)
    for p in range(pieces):
        side[p].wait_recv()
        pass_far[p].start()

    total = acc[...]
    normed = total * lax.rsqrt(jnp.mean(total * total, axis=1, keepdims=True) + head_eps)
    att[...] = (normed * hgain_ref[...]).astype(bf16).reshape(att.shape)

    def block_of(m):
        return att.at[x ^ (m & 1), :, core ^ ((m >> 1) & 1)]

    spread = [
        remote(block_of(m), th.at[m >> 1, x], ps, pr, m, device) for m, device in plane
    ]
    for copy in spread:
        copy.start()
    own = pltpu.make_async_copy(block_of(0), th.at[0, x], wsem.at[3])
    own.start()
    for copy in twins:
        copy.wait_recv()
    near.wait_recv()
    for copy in pass_own + pass_far:
        copy.wait_recv()
    own.wait()
    for copy in spread:
        copy.wait_recv()

    lefts = [
        jnp.concatenate([th[j, 0].reshape(-1, hd), th[j, 1].reshape(-1, hd)], axis=1)
        for j in range(4)
    ]
    col = min(512, width)
    for n in range(width // col):
        cut = pl.ds(n * col, col)
        mix[:, cut] = functools.reduce(
            jnp.add,
            [jnp.dot(lefts[j], owf[j, :, cut], preferred_element_type=f32) for j in range(4)],
        )
    hidden = layer_norm(
        residual_scale * res_ref[...].reshape(2 * row_count, width).astype(f32) + mix[...],
        g1_ref[...],
        b1_ref[...],
    ).astype(bf16)
    hid_ref[...] = hidden.reshape(2, row_count, width)
    chosen = [
        selection(ids_ref[yy], sp, capacity, experts),
        selection(ids_ref[1 - yy], sp, capacity, experts),
    ]
    pick = [functools.reduce(jnp.add, one).astype(bf16) for one in chosen]
    for n in range(width // col):
        cut = pl.ds(n * col, col)
        for r, many in ((0, experts), (1, dup)):
            picked = (
                jnp.dot(
                    pick[r][: many * capacity],
                    hid_ref[yy if r == 0 else 1 - yy, :, cut],
                    preferred_element_type=f32,
                )
                .astype(bf16)
                .reshape(many, capacity, col)
            )
            rows[0, 0, r, :, cut] = picked[0]
            out_ref[1:many, r, :, cut] = picked[1:]

    inner = jnp.logical_and(z > 0, has_next)
    flip = jnp.where(inner, 2, 0)

    def place(i):
        return i if i < half_dup else half_dup + ((i - half_dup) ^ flip)

    def partner(i):
        return (sp ^ i, tp)

    def send(i):
        if isinstance(i, int) and i < dup:
            return remote(out_ref.at[i], rows.at[i, 0], s0, r0, i, partner(i))
        return remote(out_ref.at[i, 0], rows.at[i, 0, 0], s0, r0, i, partner(i))

    def to_y(i):
        return remote(rows.at[i, 0, 0], rows.at[i, 0, 1], s1, r1, i, across)

    def to_core(i):
        if isinstance(i, int) and i < dup:
            return remote(rows.at[i, 0], rows.at[i, 1], s2, r2, i, beside)
        return remote(rows.at[i, 0, 0], rows.at[i, 1, 0], s2, r2, i, beside)

    def relay(i):
        return remote(rows.at[i, 0, 1], rows.at[i, 1, 1], s3, r3, i, beside)

    def swap_cores(i):
        return remote(part.at[i, 1], duo.at[i], s4, r4, i, beside)

    def sums(i):
        return remote(ysend.at[i - half_dup], yrecv.at[i - half_dup], s5, r5, i, across)

    def back(i):
        if isinstance(i, int) and i < half_dup:
            return remote(fin.at[i], ret.at[i], s6, r6, i, partner(i))
        return remote(fin_far.at[i - half_dup], ret_far.at[i - half_dup], s6, r6, i, partner(i))

    closing = [
        remote(csend.at[:, pl.ds(h * (width // 2), width // 2)],
               crecv.at[:, pl.ds(h * (width // 2), width // 2)], cs, cr, h, across)
        for h in range(2)
    ]
    def dispatch(i):
        send(i).start()

    tile, wide_col = min(256, units), min(512, width)
    gates_in, downs_in = units // tile, width // wide_col

    def enter(i):
        if i:
            send(place(i)).wait_recv()
        if i >= dup:
            to_y(place(i)).start()
        to_core(place(i)).start()

    def onward(i):
        if i >= dup:
            to_y(place(i)).wait_recv()
            relay(place(i)).start()

    def gather(g):
        for i in (2 * g, 2 * g + 1):
            to_core(place(i)).wait_recv()
            if i >= dup:
                relay(place(i)).wait_recv()

    def hidden_units(g, n):
        cut = pl.ds(n * tile, tile)
        given = rows[pl.ds(place(2 * g), 2)].reshape(-1, width)
        gate = jnp.dot(given, wg[:, cut], preferred_element_type=f32)
        up = jnp.dot(given, wu[:, cut], preferred_element_type=f32)
        act[:, cut] = (gate / (1.0 + jnp.exp(-gate)) * up).astype(bf16)

    def back_down(g, n):
        cut = pl.ds(n * wide_col, wide_col)
        down = jnp.dot(act[...], wd[:, cut], preferred_element_type=f32).astype(bf16)
        part[pl.ds(place(2 * g), 2), :, :, :, cut] = down.reshape(2, 2, 2, capacity, wide_col)

    def pair_up(i):
        swap_cores(place(i)).start()

    def cross(i):
        at = place(i)
        swap_cores(at).wait_recv()
        ysend[at - half_dup] = (part[at, 0, 1].astype(f32) + duo[at, 1].astype(f32)).astype(bf16)
        sums(at).start()

    def finish(i):
        at = place(i)
        if i >= half_dup:
            sums(at).wait_recv()
            fin_far[at - half_dup] = (
                part[at, 0, 0].astype(f32)
                + duo[at, 0].astype(f32)
                + yrecv[at - half_dup].astype(f32)
            ).astype(bf16)
        else:
            swap_cores(at).wait_recv()
            total = (part[at, 0].astype(f32) + duo[at].astype(f32)).astype(bf16)
            if i == 0:
                ret[0] = total
                return
            fin[i] = total
        back(at).start()

    def mixing_of(r, lead, many):
        logits = log_ref[yy if r == 0 else 1 - yy]
        high = jnp.max(logits, axis=0, keepdims=True)
        grown = jnp.exp(logits - high)
        gates = grown / jnp.sum(grown, axis=0, keepdims=True)
        mixing = functools.reduce(
            jnp.add,
            [
                one[lead * capacity : (lead + many) * capacity] * gates[k : k + 1, :]
                for k, one in enumerate(chosen[r])
            ],
        ).T
        top = mixing.astype(bf16)
        return top, (mixing - top.astype(f32)).astype(bf16)

    def mixed(parts, given):
        top, low = parts
        return jnp.dot(top, given, preferred_element_type=f32) + jnp.dot(
            low, given, preferred_element_type=f32
        )

    slots = half_dup * capacity

    def combine():
        ours, twin = mixing_of(0, 0, half_dup), mixing_of(1, 0, half_dup)
        for i in range(1, half_dup):
            back(i).wait_recv()
        for n in range(width // col):
            cut = pl.ds(n * col, col)
            csend[:, cut] = mixed(twin, ret[:, 1, :, cut].reshape(slots, col)).astype(bf16)
            mix[:row_count, cut] = mixed(ours, ret[:, 0, :, cut].reshape(slots, col))
        for copy in closing:
            copy.start()

    def close():
        for copy in closing:
            copy.wait_recv()
        mix[:row_count] = mix[:row_count] + crecv[...].astype(f32)

    def weights_in():
        for copy in weights:
            copy.wait()

    acts = {
        "F": enter, "R": onward, "G": gather, "P": pair_up, "X": cross, "N": finish,
        "U": hidden_units, "D": back_down, "W": weights_in, "S": dispatch, "K": combine, "L": close,
    }

    def run(token):
        acts[token[0]](*[int(v) for v in token[1:]])

    for number, token in enumerate(plan_of(gates_in, downs_in)):
        run(token)

    far = mixing_of(0, half_dup, experts - half_dup)
    for i in range(half_dup, experts):
        back(i).wait_recv()
    for n in range(width // col):
        cut = pl.ds(n * col, col)
        mix[:row_count, cut] = mix[:row_count, cut] + mixed(
            far, ret_far[:, :, cut].reshape(slots, col)
        )
    y_ref[...] = layer_norm(
        residual_scale * hid_ref[yy].astype(f32) + mix[:row_count], g2_ref[...], b2_ref[...]
    ).astype(bf16)
    leave = pltpu.make_async_copy(y_ref, y_hbm, wsem.at[3])
    leave.start()
    for copy in swaps + twins + wide + side + [near] + pass_own + pass_far + spread + closing:
        copy.wait_send()
    for i in range(experts):
        if i:
            send(i).wait_send()
            back(i).wait_send()
        to_core(i).wait_send()
        swap_cores(i).wait_send()
        if i >= dup:
            to_y(i).wait_send()
            relay(i).wait_send()
        if i >= half_dup:
            sums(i).wait_send()
    for d in range(chain - 1):

        @pl.when(jnp.logical_and(d <= z, has_next))
        def _(d=d):
            for h in range(2):
                for part_of in range(2):
                    hop(d, part_of, h).wait_send()

    leave.wait()


def fused(
    queries, keys, values, score_offset, head_gain, out_weight, residual, ln1_gain, ln1_bias,
    expert_ids, route_logits, gate_weight, up_weight, down_weight, ln2_gain, ln2_bias,
):
    experts = lax.axis_size("sp")
    tok, hd = queries.shape[0], head_gain.shape[0]
    row_count, width = residual.shape
    top_count = expert_ids.shape[1]
    capacity = max(2, 2 * top_count * row_count // experts)
    chain = experts // 2
    span = 2 * tok
    pieces, dup = 4, 2
    units = gate_weight.shape[2]
    hbm = pl.BlockSpec(memory_space=pl.ANY)
    dma = lambda n: pltpu.SemaphoreType.DMA((n,))
    limit = 62 * 1024 * 1024
    block = lambda *lead: pltpu.VMEM((*lead, capacity, width), bf16)
    line = lambda n: pltpu.VMEM((1, n), f32)
    n = experts
    return pl.pallas_call(
        functools.partial(layer_kernel, chain, experts, capacity, pieces, dup),
        out_shape=jax.ShapeDtypeStruct((row_count, width), bf16),
        in_specs=[hbm] * 16,
        out_specs=hbm,
        scratch_shapes=[
            pltpu.SMEM(score_offset.shape, f32),
            line(hd), line(width), line(width), line(width), line(width),
            pltpu.VMEM((2, top_count, row_count), jnp.int32),
            pltpu.VMEM((2, top_count, row_count), f32),
            pltpu.VMEM((2, row_count, width), bf16),
            pltpu.VMEM((3, tok, hd), bf16),
            pltpu.VMEM((row_count, width), bf16),
            pltpu.VMEM((2, row_count, width), bf16),
            block(n, 2),
            pltpu.VMEM((chain, 2, span, hd), bf16),
            pltpu.VMEM((span, hd), bf16),
            pltpu.VMEM((span, hd), f32),
            pltpu.VMEM((span, 1), f32),
            pltpu.VMEM((min(256, tok), min(256, tok)), bf16),
            pltpu.VMEM((2, 2, 2, row_count, hd), bf16),
            pltpu.VMEM((4, 2, 2, row_count, hd), bf16),
            pltpu.VMEM((4, out_weight.shape[0], width), bf16),
            pltpu.VMEM((2 * row_count, width), f32),
            block(n, 2, 2),
            pltpu.VMEM((width, units), bf16),
            pltpu.VMEM((width, units), bf16),
            pltpu.VMEM((units, width), bf16),
            pltpu.VMEM((8 * capacity, units), bf16),
            block(n, 2, 2), block(n, 2), block(n // 2), block(n // 2),
            block(n // 2, 2), block(n // 2), block(n // 2, 2), block(n // 2),
            pltpu.VMEM((row_count, width), bf16), pltpu.VMEM((row_count, width), bf16),
            dma(16), dma(3), dma(3), dma(4 * chain), dma(4 * chain), dma(8), dma(8),
            dma(4 * pieces + 1), dma(4 * pieces + 1),
            dma(4),
            dma(n), dma(n), dma(n), dma(n), dma(n), dma(n), dma(n), dma(n),
            dma(n), dma(n), dma(n), dma(n), dma(n), dma(n), dma(3), dma(3), dma(2), dma(2),
        ],
        compiler_params=pltpu.CompilerParams(
            collective_id=0, has_side_effects=True, vmem_limit_bytes=limit
        ),
    )(
        queries, keys, values, score_offset, head_gain[None], out_weight, residual,
        ln1_gain[None], ln1_bias[None], expert_ids.T, route_logits.T,
        ln2_gain[None], ln2_bias[None], gate_weight, up_weight, down_weight,
    )


def program_for(*args):
    queries, head_gain, residual, ids = args[0], args[4], args[6], args[9]
    experts = lax.axis_size("sp")
    capacity = max(2, 2 * ids.shape[1] * residual.shape[0] // experts)
    rows_ok = capacity % 16 == 0 and residual.shape[0] % 16 == 0
    heads_ok = queries.shape[1] == 2 * head_gain.shape[0] and head_gain.shape[0] % 128 == 0
    mesh_ok = lax.axis_size("tp") == 4 and experts == 8
    whole = queries.shape[0] % 128 == 0 and args[11].shape[0] == 1
    if rows_ok and heads_ok and mesh_ok and whole:
        return fused(*args)
    return on_device(*args)


def solution(mesh):
    in_specs = (
        P("sp", "tp"),
        P("sp", "tp"),
        P("sp", "tp"),
        P("tp"),
        P(),
        P("tp", None),
        P(("sp", "tp"), None),
        P(),
        P(),
        P(("sp", "tp"), None),
        P(("sp", "tp"), None),
        P("sp", None, "tp"),
        P("sp", None, "tp"),
        P("sp", "tp", None),
        P(),
        P(),
    )
    out_specs = P(("sp", "tp"), None)
    return jax.shard_map(
        program_for, mesh=mesh, in_specs=in_specs, out_specs=out_specs, check_vma=False
    )
```

```python
import functools
import jax
import jax.numpy as jnp
from jax import lax
from jax.experimental import pallas as pl
from jax.experimental.pallas import tpu as pltpu
from jax.sharding import PartitionSpec as P

residual_scale = 8.0**0.25
norm_eps = 1e-05
head_eps = 1e-06


def layer_norm(inputs, gain, shift):
    mean_value = jnp.mean(inputs, axis=-1, keepdims=True)
    centred = inputs - mean_value
    variance = jnp.mean(centred * centred, axis=-1, keepdims=True)
    return centred * lax.rsqrt(variance + norm_eps) * gain + shift


def attend(query_rows, first_pos, key_rows, value_rows, score_offset, head_gain, key_span):
    query_count = query_rows.shape[0]
    heads = score_offset.shape[0]
    head_dim = query_rows.shape[1] // heads
    query_heads = query_rows.reshape(query_count, heads, head_dim)
    query_pos = first_pos + jnp.arange(query_count, dtype=jnp.int32)
    last_block = (first_pos + query_count - 1) // key_span
    scale = head_dim ** (-0.5)

    def turn(step, carry):
        totals, survive = carry
        block_index = last_block - step
        key_tile_block = lax.dynamic_slice_in_dim(
            key_rows, block_index * key_span, key_span, 0
        ).reshape(key_span, heads, head_dim)
        value_block = lax.dynamic_slice_in_dim(
            value_rows, block_index * key_span, key_span, 0
        ).reshape(key_span, heads, head_dim)
        scores = (
            jnp.einsum(
                "qhd,khd->hqk", query_heads, key_tile_block, preferred_element_type=jnp.float32
            )
            * scale
            - score_offset[:, None, None]
        )
        key_pos = block_index * key_span + jnp.arange(key_span, dtype=jnp.int32)
        causal = (key_pos[None, :] < query_pos[:, None])[None]
        log_keep = jnp.where(causal, jax.nn.log_sigmoid(-scores), 0.0)
        tail_sum = lax.cumsum(log_keep, axis=2, reverse=True) - log_keep
        weight_values = jnp.where(
            causal, jnp.exp(jax.nn.log_sigmoid(scores) + tail_sum + survive[:, :, None]), 0.0
        ).astype(jnp.bfloat16)
        totals = totals + jnp.einsum(
            "hqk,khd->qhd", weight_values, value_block, preferred_element_type=jnp.float32
        )
        return (totals, survive + jnp.sum(log_keep, axis=2))

    start_carry = (
        jnp.zeros((query_count, heads, head_dim), jnp.float32),
        jnp.zeros((heads, query_count), jnp.float32),
    )
    totals, _ = lax.fori_loop(0, last_block + 1, turn, start_carry)
    square_mean = jnp.mean(totals * totals, axis=-1, keepdims=True)
    normed = totals * lax.rsqrt(square_mean + head_eps) * head_gain
    return normed.reshape(query_count, heads * head_dim).astype(jnp.bfloat16)


def on_device(
    queries,
    keys,
    values,
    score_offset,
    head_gain,
    out_weight,
    residual,
    ln1_gain,
    ln1_bias,
    expert_ids,
    route_logits,
    gate_weight,
    up_weight,
    down_weight,
    ln2_gain,
    ln2_bias,
):
    sp_index = lax.axis_index("sp")
    tok_dev = queries.shape[0]
    gathered_keys, gathered_values = (
        lax.all_gather(keys, "sp", axis=0, tiled=True),
        lax.all_gather(values, "sp", axis=0, tiled=True),
    )
    key_span = gathered_keys.shape[0]
    while key_span > 1024 and key_span % 2 == 0:
        key_span = key_span // 2
    first_own = sp_index * tok_dev
    att_out = attend(
        queries, first_own, gathered_keys, gathered_values, score_offset, head_gain, key_span
    )
    row_count = residual.shape[0]
    model_width = residual.shape[1]
    token_heads = lax.all_to_all(att_out, "tp", split_axis=0, concat_axis=1, tiled=True)
    mixer = jnp.dot(
        token_heads,
        lax.all_gather(out_weight, "tp", axis=0, tiled=True),
        preferred_element_type=jnp.float32,
    )
    hidden_in = layer_norm(
        residual_scale * residual.astype(jnp.float32) + mixer, ln1_gain, ln1_bias
    ).astype(jnp.bfloat16)
    top_count = expert_ids.shape[1]
    experts = lax.axis_size("sp")
    capacity = max(2, 2 * top_count * row_count // experts)
    flat_ids = expert_ids.reshape(-1)
    onehot = (flat_ids[:, None] == jnp.arange(experts, dtype=jnp.int32)[None, :]).astype(jnp.int32)
    slot_index = jnp.sum(jnp.cumsum(onehot, axis=0) * onehot, axis=1) - 1
    destination = flat_ids * capacity + slot_index
    send_rows = jnp.repeat(hidden_in, top_count, axis=0)
    outgoing = (
        jnp.zeros((experts * capacity, model_width), jnp.bfloat16).at[destination].set(send_rows)
    )
    outgoing = outgoing.reshape(experts, capacity, model_width)
    row_block = lax.all_gather(
        lax.all_to_all(outgoing, "sp", split_axis=0, concat_axis=0, tiled=True),
        "tp",
        axis=0,
        tiled=True,
    )
    block_count = row_block.shape[0]
    flat_rows = row_block.reshape(-1, model_width)
    gate_part = jnp.dot(flat_rows, gate_weight[0], preferred_element_type=jnp.float32)
    up_part = jnp.dot(flat_rows, up_weight[0], preferred_element_type=jnp.float32)
    active = (jax.nn.silu(gate_part) * up_part).astype(jnp.bfloat16)
    down_part = jnp.dot(active, down_weight[0], preferred_element_type=jnp.float32).astype(
        jnp.bfloat16
    )
    partials = down_part.reshape(block_count, -1, model_width)
    summed = (
        lax.psum_scatter(partials, "tp", scatter_dimension=0, tiled=True)
        .astype(jnp.float32)
        .astype(jnp.bfloat16)
    )
    returned_rows = lax.all_to_all(summed, "sp", split_axis=0, concat_axis=0, tiled=True)
    picked = returned_rows.reshape(experts * capacity, model_width)[destination].reshape(
        row_count, top_count, model_width
    )
    gates = jax.nn.softmax(route_logits, axis=-1)
    routed = jnp.sum(gates[:, :, None] * picked.astype(jnp.float32), axis=1)
    return layer_norm(
        residual_scale * hidden_in.astype(jnp.float32) + routed, ln2_gain, ln2_bias
    ).astype(jnp.bfloat16)


MESH = pl.DeviceIdType.MESH
f32 = jnp.float32
bf16 = jnp.bfloat16


def remote(src, dst, send, recv, slot, device):
    return pltpu.make_async_remote_copy(
        src_ref=src,
        dst_ref=dst,
        send_sem=send.at[slot],
        recv_sem=recv.at[slot],
        device_id=device,
        device_id_type=MESH,
    )


def selection(ids, sp, capacity, experts):
    rows = ids.shape[1]
    slot = lax.broadcasted_iota(jnp.int32, (experts * capacity, rows), 0)
    expert = slot // capacity
    place = (slot % capacity).astype(f32)
    named = [(ids[k : k + 1, :] ^ sp) == expert for k in range(ids.shape[0])]
    either = functools.reduce(jnp.logical_or, named)
    before = (
        lax.broadcasted_iota(jnp.int32, (rows, rows), 0)
        < lax.broadcasted_iota(jnp.int32, (rows, rows), 1)
    )
    rank = jnp.dot(
        either.astype(f32).astype(bf16), before.astype(f32).astype(bf16), preferred_element_type=f32
    )
    fits = rank == place
    return [jnp.where(jnp.logical_and(one, fits), 1.0, 0.0) for one in named]


def plan_of(gates_in, downs_in):
    def work(g, fill):
        units = [f"U{g}{n}" for n in range(gates_in)] + [f"D{g}{n}" for n in range(downs_in)]
        out, fill = [f"G{g}"], list(fill)
        for at, unit in enumerate(units):
            out.append(unit)
            out += fill[at * len(fill) // len(units) : (at + 1) * len(fill) // len(units)]
        return out

    plan = ["S1", "S2", "S3", "S4", "S5", "S6", "S7", "F0", "F1", "F2", "W"]
    plan += work(0, ['R2', 'F3', 'F4']) + ['P0', 'P1', 'F5', 'N0', 'N1', 'R3']
    plan += work(1, ['R4', 'F6']) + ['P2', 'P3', 'R5', 'F7', 'N2', 'N3']
    plan += work(2, ['R6']) + ['P4', 'P5', 'X4', 'X5', 'R7']
    plan += work(3, ['N4', 'N5']) + ['P6', 'P7', 'X6', 'X7', 'N6', 'N7', 'K', 'L']
    return plan


def layer_kernel(
    chain, experts, capacity, pieces, dup,
    q_hbm, k_hbm, v_hbm, off_hbm, hgain_hbm, ow_hbm, res_hbm, g1_hbm, b1_hbm, ids_hbm,
    log_hbm, g2_hbm, b2_hbm, wg_hbm, wu_hbm, wd_hbm,
    y_ref,
    off_ref, hgain_ref, g1_ref, b1_ref, g2_ref, b2_ref, ids_ref, log_ref, res_ref, give,
    hid_ref, out_ref, kv, qb, acc, surv, tri, att, th, owf, mix,
    rows, wg, wu, wd, act, part, duo, ysend, yrecv, fin, fin_far, ret, ret_far, csend, crecv,
    lsem, xs, xr, zs, zr, ps, pr, ws, wr,
    wsem, s0, r0, s1, r1, s2, r2, s3, r3, s4, r4, s5, r5, s6, r6, es, er, cs, cr,
):
    sp, tp = lax.axis_index("sp"), lax.axis_index("tp")
    z, x = sp // 2, sp % 2
    yy, core = tp // 2, tp % 2
    tok, hd = q_hbm.shape[0], hgain_ref.shape[1]
    row_count, width = res_hbm.shape
    units = wg.shape[1]
    span = 2 * tok
    has_next = z + 1 < chain
    half_dup = experts // 2

    plane = [(m, (sp ^ (m & 1), tp ^ (m >> 1))) for m in range(1, 8)]
    barrier = pltpu.get_barrier_semaphore()
    others = [(sp ^ i, tp) for i in range(1, experts)]
    greeted = [device for _, device in plane] + others[1:]
    for device in greeted:
        pl.semaphore_signal(barrier, inc=1, device_id=device, device_id_type=MESH)
    mine = pl.ds(pl.multiple_of(x * tok, tok), tok)
    theirs = pl.ds(pl.multiple_of((1 - x) * tok, tok), tok)
    own_cols = pl.ds(pl.multiple_of(x * hd, hd), hd)
    peer_cols = pl.ds(pl.multiple_of((1 - x) * hd, hd), hd)
    fetches = [
        (k_hbm.at[:, peer_cols], give.at[0]),
        (v_hbm.at[:, peer_cols], give.at[1]),
        (k_hbm.at[:, own_cols], kv.at[0, 0, mine]),
        (v_hbm.at[:, own_cols], kv.at[0, 1, mine]),
        (q_hbm.at[:, peer_cols], give.at[2]),
        (ow_hbm, owf.at[0]),
        (q_hbm.at[:, own_cols], qb.at[mine]),
        (ids_hbm, ids_ref.at[yy]),
        (log_hbm, log_ref.at[yy]),
        (res_hbm, res_ref.at[yy]),
        (off_hbm, off_ref),
        (hgain_hbm, hgain_ref),
        (g1_hbm, g1_ref),
        (b1_hbm, b1_ref),
        (g2_hbm, g2_ref),
        (b2_hbm, b2_ref),
    ]
    local = [
        pltpu.make_async_copy(src, dst, lsem.at[n]) for n, (src, dst) in enumerate(fetches)
    ]
    weights = [
        pltpu.make_async_copy(wg_hbm.at[0], wg, wsem.at[0]),
        pltpu.make_async_copy(wu_hbm.at[0], wu, wsem.at[1]),
        pltpu.make_async_copy(wd_hbm.at[0], wd, wsem.at[2]),
    ]
    for copy in local + weights:
        copy.start()

    tri[...] = jnp.where(
        lax.broadcasted_iota(jnp.int32, tri.shape, 0)
        > lax.broadcasted_iota(jnp.int32, tri.shape, 1),
        -1.0,
        0.0,
    ).astype(bf16)
    acc[...] = jnp.zeros_like(acc)
    surv[...] = jnp.zeros_like(surv)
    pl.semaphore_wait(barrier, len(greeted))

    pair = (sp ^ 1, tp)
    swaps = [
        remote(give.at[0], kv.at[0, 0, mine], xs, xr, 0, pair),
        remote(give.at[1], kv.at[0, 1, mine], xs, xr, 1, pair),
        remote(give.at[2], qb.at[mine], xs, xr, 2, pair),
    ]
    for n, at in enumerate((0, 1)):
        local[at].wait()
        swaps[n].start()
    across, beside = (sp, tp ^ 2), (sp, tp ^ 1)
    half = owf.shape[1] // 2
    strip = half // pieces

    def strip_of(side, p):
        return pl.ds(pl.multiple_of(side * half + p * strip, strip), strip)

    def weight_copy(src, dst, side, p, slot, device):
        at = strip_of(side, p)
        return remote(owf.at[src, at], owf.at[dst, at], ws, wr, slot, device)

    near = remote(owf.at[0], owf.at[1], ws, wr, 4 * pieces, beside)
    wide = [weight_copy(0, 2, x, p, p, across) for p in range(pieces)]
    side = [weight_copy(2, 2, x, p, pieces + p, pair) for p in range(pieces)]
    pass_own = [weight_copy(2, 3, x, p, 2 * pieces + p, beside) for p in range(pieces)]
    pass_far = [weight_copy(2, 3, 1 - x, p, 3 * pieces + p, beside) for p in range(pieces)]
    twins = [
        remote(ids_ref.at[yy], ids_ref.at[yy], es, er, 0, across),
        remote(log_ref.at[yy], log_ref.at[yy], es, er, 1, across),
        remote(res_ref.at[yy], res_ref.at[yy], es, er, 2, across),
    ]

    def weight_step(p):
        wide[p].wait_recv()
        side[p].start()
        pass_own[p].start()

    def hop(d, part, h):
        where = mine if h == 0 else theirs
        slot = (d * 2 + part) * 2 + h
        return pltpu.make_async_remote_copy(
            src_ref=kv.at[d, part, where],
            dst_ref=kv.at[d + 1, part, where],
            send_sem=zs.at[slot],
            recv_sem=zr.at[slot],
            device_id=(sp + 2, tp),
            device_id_type=MESH,
        )

    log2e = 1.4426950408889634
    scale = hd ** (-0.5) * log2e
    k_tile = tri.shape[0]

    def block(d):
        offset = jnp.where(x == 0, off_ref[0], off_ref[1]) * log2e
        for kb in reversed(range(span // k_tile)):
            lead = kb * k_tile if d == 0 else 0
            at = pl.ds(lead, span - lead)
            query = qb[at, :]
            out, survive = acc[at, :], surv[at, :]
            keys = kv[d, 0, pl.ds(kb * k_tile, k_tile), :]
            scores = (
                lax.dot_general(
                    query, keys, (((1,), (1,)), ((), ())), preferred_element_type=f32
                )
                * scale
                - offset
            )
            drop = jnp.maximum(scores, 0.0) + log2e * jnp.log(1.0 + jnp.exp2(-jnp.abs(scores)))
            take = scores - drop
            if d == 0:
                causal = (
                    lax.broadcasted_iota(jnp.int32, scores.shape, 1)
                    < lax.broadcasted_iota(jnp.int32, scores.shape, 0)
                )
                drop = jnp.where(causal, drop, 0.0)
            top = drop.astype(bf16)
            low = (drop - top.astype(f32)).astype(bf16)
            tail = jnp.dot(top, tri[...], preferred_element_type=f32) + jnp.dot(
                low, tri[...], preferred_element_type=f32
            )
            weight = jnp.exp2(take + tail + survive)
            if d == 0:
                weight = jnp.where(causal, weight, 0.0)
            acc[at, :] = out + jnp.dot(
                weight.astype(bf16),
                kv[d, 1, pl.ds(kb * k_tile, k_tile), :],
                preferred_element_type=f32,
            )
            surv[at, :] = survive + (tail[:, :1] - drop[:, :1])

    local[2].wait()
    local[3].wait()

    @pl.when(has_next)
    def _():
        hop(0, 0, 0).start()
        hop(0, 1, 0).start()

    local[4].wait()
    swaps[2].start()
    local[7].wait()
    twins[0].start()
    local[8].wait()
    twins[1].start()
    local[5].wait()
    for copy in wide:
        copy.start()
    local[9].wait()
    twins[2].start()
    near.start()

    def receive(d, h):
        for part in range(2):
            hop(d - 1, part, h).wait_recv()
            if d + 1 < chain:

                @pl.when(has_next)
                def _():
                    hop(d, part, h).start()

    @pl.when(z >= 1)
    def _():
        receive(1, 0)

    swaps[0].wait_recv()
    swaps[1].wait_recv()

    @pl.when(has_next)
    def _():
        hop(0, 0, 1).start()
        hop(0, 1, 1).start()

    for at in (6, 10, 11, 12, 13, 14, 15):
        local[at].wait()
    swaps[2].wait_recv()
    weight_step(0)
    block(0)
    weight_step(1)
    for d in range(1, chain):

        @pl.when(d <= z)
        def _(d=d):
            if d > 1:
                receive(d, 0)
            receive(d, 1)
            block(d)

        if d == 1:
            for p in range(2, pieces):
                weight_step(p)
    for p in range(pieces):
        side[p].wait_recv()
        pass_far[p].start()

    total = acc[...]
    normed = total * lax.rsqrt(jnp.mean(total * total, axis=1, keepdims=True) + head_eps)
    att[...] = (normed * hgain_ref[...]).astype(bf16).reshape(att.shape)

    def block_of(m):
        return att.at[x ^ (m & 1), :, core ^ ((m >> 1) & 1)]

    spread = [
        remote(block_of(m), th.at[m >> 1, x], ps, pr, m, device) for m, device in plane
    ]
    for copy in spread:
        copy.start()
    own = pltpu.make_async_copy(block_of(0), th.at[0, x], wsem.at[3])
    own.start()
    for copy in twins:
        copy.wait_recv()
    near.wait_recv()
    for copy in pass_own + pass_far:
        copy.wait_recv()
    own.wait()
    for copy in spread:
        copy.wait_recv()

    lefts = [
        jnp.concatenate([th[j, 0].reshape(-1, hd), th[j, 1].reshape(-1, hd)], axis=1)
        for j in range(4)
    ]
    col = min(512, width)
    for n in range(width // col):
        cut = pl.ds(n * col, col)
        mix[:, cut] = functools.reduce(
            jnp.add,
            [jnp.dot(lefts[j], owf[j, :, cut], preferred_element_type=f32) for j in range(4)],
        )
    hidden = layer_norm(
        residual_scale * res_ref[...].reshape(2 * row_count, width).astype(f32) + mix[...],
        g1_ref[...],
        b1_ref[...],
    ).astype(bf16)
    hid_ref[...] = hidden.reshape(2, row_count, width)
    chosen = [
        selection(ids_ref[yy], sp, capacity, experts),
        selection(ids_ref[1 - yy], sp, capacity, experts),
    ]
    pick = [functools.reduce(jnp.add, one).astype(bf16) for one in chosen]
    for n in range(width // col):
        cut = pl.ds(n * col, col)
        for r, many in ((0, experts), (1, dup)):
            picked = (
                jnp.dot(
                    pick[r][: many * capacity],
                    hid_ref[yy if r == 0 else 1 - yy, :, cut],
                    preferred_element_type=f32,
                )
                .astype(bf16)
                .reshape(many, capacity, col)
            )
            rows[0, 0, r, :, cut] = picked[0]
            out_ref[1:many, r, :, cut] = picked[1:]

    inner = jnp.logical_and(z > 0, has_next)
    flip = jnp.where(inner, 2, 0)

    def place(i):
        return i if i < half_dup else half_dup + ((i - half_dup) ^ (2 - flip))

    def partner(i):
        return (sp ^ i, tp)

    def send(i):
        if isinstance(i, int) and i < dup:
            return remote(out_ref.at[i], rows.at[i, 0], s0, r0, i, partner(i))
        return remote(out_ref.at[i, 0], rows.at[i, 0, 0], s0, r0, i, partner(i))

    def to_y(i):
        return remote(rows.at[i, 0, 0], rows.at[i, 0, 1], s1, r1, i, across)

    def to_core(i):
        if isinstance(i, int) and i < dup:
            return remote(rows.at[i, 0], rows.at[i, 1], s2, r2, i, beside)
        return remote(rows.at[i, 0, 0], rows.at[i, 1, 0], s2, r2, i, beside)

    def relay(i):
        return remote(rows.at[i, 0, 1], rows.at[i, 1, 1], s3, r3, i, beside)

    def swap_cores(i):
        return remote(part.at[i, 1], duo.at[i], s4, r4, i, beside)

    def sums(i):
        return remote(ysend.at[i - half_dup], yrecv.at[i - half_dup], s5, r5, i, across)

    def back(i):
        if isinstance(i, int) and i < half_dup:
            return remote(fin.at[i], ret.at[i], s6, r6, i, partner(i))
        return remote(fin_far.at[i - half_dup], ret_far.at[i - half_dup], s6, r6, i, partner(i))

    closing = [
        remote(csend.at[:, pl.ds(h * (width // 2), width // 2)],
               crecv.at[:, pl.ds(h * (width // 2), width // 2)], cs, cr, h, across)
        for h in range(2)
    ]
    def dispatch(i):
        send(i if i < half_dup else half_dup + ((i - half_dup) ^ (2 - flip))).start()

    tile, wide_col = min(256, units), min(512, width)
    gates_in, downs_in = units // tile, width // wide_col

    def enter(i):
        if i:
            send(place(i)).wait_recv()
        if i >= dup:
            to_y(place(i)).start()
        to_core(place(i)).start()

    def onward(i):
        if i >= dup:
            to_y(place(i)).wait_recv()
            relay(place(i)).start()

    def gather(g):
        for i in (2 * g, 2 * g + 1):
            to_core(place(i)).wait_recv()
            if i >= dup:
                relay(place(i)).wait_recv()

    def hidden_units(g, n):
        cut = pl.ds(n * tile, tile)
        given = rows[pl.ds(place(2 * g), 2)].reshape(-1, width)
        gate = jnp.dot(given, wg[:, cut], preferred_element_type=f32)
        up = jnp.dot(given, wu[:, cut], preferred_element_type=f32)
        act[:, cut] = (gate / (1.0 + jnp.exp(-gate)) * up).astype(bf16)

    def back_down(g, n):
        cut = pl.ds(n * wide_col, wide_col)
        down = jnp.dot(act[...], wd[:, cut], preferred_element_type=f32).astype(bf16)
        part[pl.ds(place(2 * g), 2), :, :, :, cut] = down.reshape(2, 2, 2, capacity, wide_col)

    def pair_up(i):
        swap_cores(place(i)).start()

    def cross(i):
        at = place(i)
        swap_cores(at).wait_recv()
        ysend[at - half_dup] = (part[at, 0, 1].astype(f32) + duo[at, 1].astype(f32)).astype(bf16)
        sums(at).start()

    def finish(i):
        at = place(i)
        if i >= half_dup:
            sums(at).wait_recv()
            fin_far[at - half_dup] = (
                part[at, 0, 0].astype(f32)
                + duo[at, 0].astype(f32)
                + yrecv[at - half_dup].astype(f32)
            ).astype(bf16)
        else:
            swap_cores(at).wait_recv()
            total = (part[at, 0].astype(f32) + duo[at].astype(f32)).astype(bf16)
            if i == 0:
                ret[0] = total
                return
            fin[i] = total
        back(at).start()

    def mixing_of(r, lead, many):
        logits = log_ref[yy if r == 0 else 1 - yy]
        high = jnp.max(logits, axis=0, keepdims=True)
        grown = jnp.exp(logits - high)
        gates = grown / jnp.sum(grown, axis=0, keepdims=True)
        mixing = functools.reduce(
            jnp.add,
            [
                one[lead * capacity : (lead + many) * capacity] * gates[k : k + 1, :]
                for k, one in enumerate(chosen[r])
            ],
        ).T
        top = mixing.astype(bf16)
        return top, (mixing - top.astype(f32)).astype(bf16)

    def mixed(parts, given):
        top, low = parts
        return jnp.dot(top, given, preferred_element_type=f32) + jnp.dot(
            low, given, preferred_element_type=f32
        )

    slots = half_dup * capacity

    def combine():
        ours, twin = mixing_of(0, 0, half_dup), mixing_of(1, 0, half_dup)
        for i in range(1, half_dup):
            back(i).wait_recv()
        for n in range(width // col):
            cut = pl.ds(n * col, col)
            csend[:, cut] = mixed(twin, ret[:, 1, :, cut].reshape(slots, col)).astype(bf16)
            mix[:row_count, cut] = mixed(ours, ret[:, 0, :, cut].reshape(slots, col))
        for copy in closing:
            copy.start()

    def close():
        for copy in closing:
            copy.wait_recv()
        mix[:row_count] = mix[:row_count] + crecv[...].astype(f32)

    def weights_in():
        for copy in weights:
            copy.wait()

    acts = {
        "F": enter, "R": onward, "G": gather, "P": pair_up, "X": cross, "N": finish,
        "U": hidden_units, "D": back_down, "W": weights_in, "S": dispatch, "K": combine, "L": close,
    }

    def run(token):
        acts[token[0]](*[int(v) for v in token[1:]])

    for number, token in enumerate(plan_of(gates_in, downs_in)):
        run(token)

    far = mixing_of(0, half_dup, experts - half_dup)
    for i in range(half_dup, experts):
        back(i).wait_recv()
    for n in range(width // col):
        cut = pl.ds(n * col, col)
        mix[:row_count, cut] = mix[:row_count, cut] + mixed(
            far, ret_far[:, :, cut].reshape(slots, col)
        )
    y_ref[...] = layer_norm(
        residual_scale * hid_ref[yy].astype(f32) + mix[:row_count], g2_ref[...], b2_ref[...]
    ).astype(bf16)
    for copy in swaps + twins + wide + side + [near] + pass_own + pass_far + spread + closing:
        copy.wait_send()
    for i in range(experts):
        if i:
            send(i).wait_send()
            back(i).wait_send()
        to_core(i).wait_send()
        swap_cores(i).wait_send()
        if i >= dup:
            to_y(i).wait_send()
            relay(i).wait_send()
        if i >= half_dup:
            sums(i).wait_send()
    for d in range(chain - 1):

        @pl.when(jnp.logical_and(d <= z, has_next))
        def _(d=d):
            for h in range(2):
                for part_of in range(2):
                    hop(d, part_of, h).wait_send()


def fused(
    queries, keys, values, score_offset, head_gain, out_weight, residual, ln1_gain, ln1_bias,
    expert_ids, route_logits, gate_weight, up_weight, down_weight, ln2_gain, ln2_bias,
):
    experts = lax.axis_size("sp")
    tok, hd = queries.shape[0], head_gain.shape[0]
    row_count, width = residual.shape
    top_count = expert_ids.shape[1]
    capacity = max(2, 2 * top_count * row_count // experts)
    chain = experts // 2
    span = 2 * tok
    pieces, dup = 4, 2
    units = gate_weight.shape[2]
    hbm = pl.BlockSpec(memory_space=pl.ANY)
    dma = lambda n: pltpu.SemaphoreType.DMA((n,))
    limit = 56 * 1024 * 1024
    block = lambda *lead: pltpu.VMEM((*lead, capacity, width), bf16)
    line = lambda n: pltpu.VMEM((1, n), f32)
    n = experts
    return pl.pallas_call(
        functools.partial(layer_kernel, chain, experts, capacity, pieces, dup),
        out_shape=pltpu.VMEM((row_count, width), bf16),
        in_specs=[hbm] * 16,
        out_specs=pl.BlockSpec(memory_space=pltpu.VMEM),
        scratch_shapes=[
            pltpu.SMEM(score_offset.shape, f32),
            line(hd), line(width), line(width), line(width), line(width),
            pltpu.VMEM((2, top_count, row_count), jnp.int32),
            pltpu.VMEM((2, top_count, row_count), f32),
            pltpu.VMEM((2, row_count, width), bf16),
            pltpu.VMEM((3, tok, hd), bf16),
            pltpu.VMEM((2, row_count, width), bf16),
            block(n, 2),
            pltpu.VMEM((chain, 2, span, hd), bf16),
            pltpu.VMEM((span, hd), bf16),
            pltpu.VMEM((span, hd), f32),
            pltpu.VMEM((span, 1), f32),
            pltpu.VMEM((min(256, tok), min(256, tok)), bf16),
            pltpu.VMEM((2, 2, 2, row_count, hd), bf16),
            pltpu.VMEM((4, 2, 2, row_count, hd), bf16),
            pltpu.VMEM((4, out_weight.shape[0], width), bf16),
            pltpu.VMEM((2 * row_count, width), f32),
            block(n, 2, 2),
            pltpu.VMEM((width, units), bf16),
            pltpu.VMEM((width, units), bf16),
            pltpu.VMEM((units, width), bf16),
            pltpu.VMEM((8 * capacity, units), bf16),
            block(n, 2, 2), block(n, 2), block(n // 2), block(n // 2),
            block(n // 2, 2), block(n // 2), block(n // 2, 2), block(n // 2),
            pltpu.VMEM((row_count, width), bf16), pltpu.VMEM((row_count, width), bf16),
            dma(16), dma(3), dma(3), dma(4 * chain), dma(4 * chain), dma(8), dma(8),
            dma(4 * pieces + 1), dma(4 * pieces + 1),
            dma(4),
            dma(n), dma(n), dma(n), dma(n), dma(n), dma(n), dma(n), dma(n),
            dma(n), dma(n), dma(n), dma(n), dma(n), dma(n), dma(3), dma(3), dma(2), dma(2),
        ],
        compiler_params=pltpu.CompilerParams(
            collective_id=0, has_side_effects=True, vmem_limit_bytes=limit
        ),
    )(
        queries, keys, values, score_offset, head_gain[None], out_weight, residual,
        ln1_gain[None], ln1_bias[None], expert_ids.T, route_logits.T,
        ln2_gain[None], ln2_bias[None], gate_weight, up_weight, down_weight,
    )


def program_for(*args):
    queries, head_gain, residual, ids = args[0], args[4], args[6], args[9]
    experts = lax.axis_size("sp")
    capacity = max(2, 2 * ids.shape[1] * residual.shape[0] // experts)
    rows_ok = capacity % 16 == 0 and residual.shape[0] % 16 == 0
    heads_ok = queries.shape[1] == 2 * head_gain.shape[0] and head_gain.shape[0] % 128 == 0
    mesh_ok = lax.axis_size("tp") == 4 and experts == 8
    whole = queries.shape[0] % 128 == 0 and args[11].shape[0] == 1
    if rows_ok and heads_ok and mesh_ok and whole:
        return fused(*args)
    return on_device(*args)


def solution(mesh):
    in_specs = (
        P("sp", "tp"),
        P("sp", "tp"),
        P("sp", "tp"),
        P("tp"),
        P(),
        P("tp", None),
        P(("sp", "tp"), None),
        P(),
        P(),
        P(("sp", "tp"), None),
        P(("sp", "tp"), None),
        P("sp", None, "tp"),
        P("sp", None, "tp"),
        P("sp", "tp", None),
        P(),
        P(),
    )
    out_specs = P(("sp", "tp"), None)
    return jax.shard_map(
        program_for, mesh=mesh, in_specs=in_specs, out_specs=out_specs, check_vma=False
    )
```

```python
import functools
import jax
import jax.numpy as jnp
from jax import lax
from jax.experimental import pallas as pl
from jax.experimental.pallas import tpu as pltpu
from jax.sharding import PartitionSpec as P

residual_scale = 8.0**0.25
norm_eps = 1e-05
head_eps = 1e-06


def layer_norm(inputs, gain, shift):
    mean_value = jnp.mean(inputs, axis=-1, keepdims=True)
    centred = inputs - mean_value
    variance = jnp.mean(centred * centred, axis=-1, keepdims=True)
    return centred * lax.rsqrt(variance + norm_eps) * gain + shift


def attend(query_rows, first_pos, key_rows, value_rows, score_offset, head_gain, key_span):
    query_count = query_rows.shape[0]
    heads = score_offset.shape[0]
    head_dim = query_rows.shape[1] // heads
    query_heads = query_rows.reshape(query_count, heads, head_dim)
    query_pos = first_pos + jnp.arange(query_count, dtype=jnp.int32)
    last_block = (first_pos + query_count - 1) // key_span
    scale = head_dim ** (-0.5)

    def turn(step, carry):
        totals, survive = carry
        block_index = last_block - step
        key_tile_block = lax.dynamic_slice_in_dim(
            key_rows, block_index * key_span, key_span, 0
        ).reshape(key_span, heads, head_dim)
        value_block = lax.dynamic_slice_in_dim(
            value_rows, block_index * key_span, key_span, 0
        ).reshape(key_span, heads, head_dim)
        scores = (
            jnp.einsum(
                "qhd,khd->hqk", query_heads, key_tile_block, preferred_element_type=jnp.float32
            )
            * scale
            - score_offset[:, None, None]
        )
        key_pos = block_index * key_span + jnp.arange(key_span, dtype=jnp.int32)
        causal = (key_pos[None, :] < query_pos[:, None])[None]
        log_keep = jnp.where(causal, jax.nn.log_sigmoid(-scores), 0.0)
        tail_sum = lax.cumsum(log_keep, axis=2, reverse=True) - log_keep
        weight_values = jnp.where(
            causal, jnp.exp(jax.nn.log_sigmoid(scores) + tail_sum + survive[:, :, None]), 0.0
        ).astype(jnp.bfloat16)
        totals = totals + jnp.einsum(
            "hqk,khd->qhd", weight_values, value_block, preferred_element_type=jnp.float32
        )
        return (totals, survive + jnp.sum(log_keep, axis=2))

    start_carry = (
        jnp.zeros((query_count, heads, head_dim), jnp.float32),
        jnp.zeros((heads, query_count), jnp.float32),
    )
    totals, _ = lax.fori_loop(0, last_block + 1, turn, start_carry)
    square_mean = jnp.mean(totals * totals, axis=-1, keepdims=True)
    normed = totals * lax.rsqrt(square_mean + head_eps) * head_gain
    return normed.reshape(query_count, heads * head_dim).astype(jnp.bfloat16)


def on_device(
    queries,
    keys,
    values,
    score_offset,
    head_gain,
    out_weight,
    residual,
    ln1_gain,
    ln1_bias,
    expert_ids,
    route_logits,
    gate_weight,
    up_weight,
    down_weight,
    ln2_gain,
    ln2_bias,
):
    sp_index = lax.axis_index("sp")
    tok_dev = queries.shape[0]
    gathered_keys, gathered_values = (
        lax.all_gather(keys, "sp", axis=0, tiled=True),
        lax.all_gather(values, "sp", axis=0, tiled=True),
    )
    key_span = gathered_keys.shape[0]
    while key_span > 1024 and key_span % 2 == 0:
        key_span = key_span // 2
    first_own = sp_index * tok_dev
    att_out = attend(
        queries, first_own, gathered_keys, gathered_values, score_offset, head_gain, key_span
    )
    row_count = residual.shape[0]
    model_width = residual.shape[1]
    token_heads = lax.all_to_all(att_out, "tp", split_axis=0, concat_axis=1, tiled=True)
    mixer = jnp.dot(
        token_heads,
        lax.all_gather(out_weight, "tp", axis=0, tiled=True),
        preferred_element_type=jnp.float32,
    )
    hidden_in = layer_norm(
        residual_scale * residual.astype(jnp.float32) + mixer, ln1_gain, ln1_bias
    ).astype(jnp.bfloat16)
    top_count = expert_ids.shape[1]
    experts = lax.axis_size("sp")
    capacity = max(2, 2 * top_count * row_count // experts)
    flat_ids = expert_ids.reshape(-1)
    onehot = (flat_ids[:, None] == jnp.arange(experts, dtype=jnp.int32)[None, :]).astype(jnp.int32)
    slot_index = jnp.sum(jnp.cumsum(onehot, axis=0) * onehot, axis=1) - 1
    destination = flat_ids * capacity + slot_index
    send_rows = jnp.repeat(hidden_in, top_count, axis=0)
    outgoing = (
        jnp.zeros((experts * capacity, model_width), jnp.bfloat16).at[destination].set(send_rows)
    )
    outgoing = outgoing.reshape(experts, capacity, model_width)
    row_block = lax.all_gather(
        lax.all_to_all(outgoing, "sp", split_axis=0, concat_axis=0, tiled=True),
        "tp",
        axis=0,
        tiled=True,
    )
    block_count = row_block.shape[0]
    flat_rows = row_block.reshape(-1, model_width)
    gate_part = jnp.dot(flat_rows, gate_weight[0], preferred_element_type=jnp.float32)
    up_part = jnp.dot(flat_rows, up_weight[0], preferred_element_type=jnp.float32)
    active = (jax.nn.silu(gate_part) * up_part).astype(jnp.bfloat16)
    down_part = jnp.dot(active, down_weight[0], preferred_element_type=jnp.float32).astype(
        jnp.bfloat16
    )
    partials = down_part.reshape(block_count, -1, model_width)
    summed = (
        lax.psum_scatter(partials, "tp", scatter_dimension=0, tiled=True)
        .astype(jnp.float32)
        .astype(jnp.bfloat16)
    )
    returned_rows = lax.all_to_all(summed, "sp", split_axis=0, concat_axis=0, tiled=True)
    picked = returned_rows.reshape(experts * capacity, model_width)[destination].reshape(
        row_count, top_count, model_width
    )
    gates = jax.nn.softmax(route_logits, axis=-1)
    routed = jnp.sum(gates[:, :, None] * picked.astype(jnp.float32), axis=1)
    return layer_norm(
        residual_scale * hidden_in.astype(jnp.float32) + routed, ln2_gain, ln2_bias
    ).astype(jnp.bfloat16)


MESH = pl.DeviceIdType.MESH
f32 = jnp.float32
bf16 = jnp.bfloat16


def remote(src, dst, send, recv, slot, device):
    return pltpu.make_async_remote_copy(
        src_ref=src,
        dst_ref=dst,
        send_sem=send.at[slot],
        recv_sem=recv.at[slot],
        device_id=device,
        device_id_type=MESH,
    )


def selection(ids, sp, capacity, experts):
    rows = ids.shape[1]
    slot = lax.broadcasted_iota(jnp.int32, (experts * capacity, rows), 0)
    expert = slot // capacity
    place = (slot % capacity).astype(f32)
    named = [(ids[k : k + 1, :] ^ sp) == expert for k in range(ids.shape[0])]
    either = functools.reduce(jnp.logical_or, named)
    before = (
        lax.broadcasted_iota(jnp.int32, (rows, rows), 0)
        < lax.broadcasted_iota(jnp.int32, (rows, rows), 1)
    )
    rank = jnp.dot(
        either.astype(f32).astype(bf16), before.astype(f32).astype(bf16), preferred_element_type=f32
    )
    fits = rank == place
    return [jnp.where(jnp.logical_and(one, fits), 1.0, 0.0) for one in named]


def plan_of(gates_in, downs_in):
    def work(g, fill):
        units = [f"U{g}{n}" for n in range(gates_in)] + [f"D{g}{n}" for n in range(downs_in)]
        out, fill = [f"G{g}"], list(fill)
        for at, unit in enumerate(units):
            out.append(unit)
            out += fill[at * len(fill) // len(units) : (at + 1) * len(fill) // len(units)]
        return out

    plan = ["S1", "S2", "S3", "S4", "S5", "S6", "S7", "F0", "F1", "F2", "W"]
    plan += work(0, ['R2', 'F3', 'F4']) + ['P0', 'P1', 'F5', 'R3']
    plan += work(1, ['N0', 'N1', 'R4', 'F6']) + ['P2', 'P3', 'R5', 'F7', 'N2', 'N3']
    plan += work(2, ['R6']) + ['P4', 'P5', 'X4', 'X5', 'R7']
    plan += work(3, ['N4', 'N5']) + ['P6', 'P7', 'X6', 'X7', 'N6', 'N7', 'K', 'L']
    return plan


def layer_kernel(
    chain, experts, capacity, pieces, dup,
    q_hbm, k_hbm, v_hbm, off_hbm, hgain_hbm, ow_hbm, res_hbm, g1_hbm, b1_hbm, ids_hbm,
    log_hbm, g2_hbm, b2_hbm, wg_hbm, wu_hbm, wd_hbm,
    y_ref,
    off_ref, hgain_ref, g1_ref, b1_ref, g2_ref, b2_ref, ids_ref, log_ref, res_ref, give,
    hid_ref, out_ref, kv, qb, acc, surv, tri, att, th, owf, mix,
    rows, wg, wu, wd, act, part, duo, ysend, yrecv, fin, fin_far, ret, ret_far, csend, crecv,
    lsem, xs, xr, zs, zr, ps, pr, ws, wr,
    wsem, s0, r0, s1, r1, s2, r2, s3, r3, s4, r4, s5, r5, s6, r6, es, er, cs, cr,
):
    sp, tp = lax.axis_index("sp"), lax.axis_index("tp")
    z, x = sp // 2, sp % 2
    yy, core = tp // 2, tp % 2
    tok, hd = q_hbm.shape[0], hgain_ref.shape[1]
    row_count, width = res_hbm.shape
    units = wg.shape[1]
    span = 2 * tok
    has_next = z + 1 < chain
    half_dup = experts // 2

    plane = [(m, (sp ^ (m & 1), tp ^ (m >> 1))) for m in range(1, 8)]
    barrier = pltpu.get_barrier_semaphore()
    others = [(sp ^ i, tp) for i in range(1, experts)]
    greeted = [device for _, device in plane] + others[1:]
    for device in greeted:
        pl.semaphore_signal(barrier, inc=1, device_id=device, device_id_type=MESH)
    mine = pl.ds(pl.multiple_of(x * tok, tok), tok)
    theirs = pl.ds(pl.multiple_of((1 - x) * tok, tok), tok)
    own_cols = pl.ds(pl.multiple_of(x * hd, hd), hd)
    peer_cols = pl.ds(pl.multiple_of((1 - x) * hd, hd), hd)
    fetches = [
        (k_hbm.at[:, peer_cols], give.at[0]),
        (v_hbm.at[:, peer_cols], give.at[1]),
        (k_hbm.at[:, own_cols], kv.at[0, 0, mine]),
        (v_hbm.at[:, own_cols], kv.at[0, 1, mine]),
        (q_hbm.at[:, peer_cols], give.at[2]),
        (ow_hbm, owf.at[0]),
        (q_hbm.at[:, own_cols], qb.at[mine]),
        (ids_hbm, ids_ref.at[yy]),
        (log_hbm, log_ref.at[yy]),
        (res_hbm, res_ref.at[yy]),
        (off_hbm, off_ref),
        (hgain_hbm, hgain_ref),
        (g1_hbm, g1_ref),
        (b1_hbm, b1_ref),
        (g2_hbm, g2_ref),
        (b2_hbm, b2_ref),
    ]
    local = [
        pltpu.make_async_copy(src, dst, lsem.at[n]) for n, (src, dst) in enumerate(fetches)
    ]
    weights = [
        pltpu.make_async_copy(wg_hbm.at[0], wg, wsem.at[0]),
        pltpu.make_async_copy(wu_hbm.at[0], wu, wsem.at[1]),
        pltpu.make_async_copy(wd_hbm.at[0], wd, wsem.at[2]),
    ]
    for copy in local + weights:
        copy.start()

    tri[...] = jnp.where(
        lax.broadcasted_iota(jnp.int32, tri.shape, 0)
        > lax.broadcasted_iota(jnp.int32, tri.shape, 1),
        -1.0,
        0.0,
    ).astype(bf16)
    acc[...] = jnp.zeros_like(acc)
    surv[...] = jnp.zeros_like(surv)
    pl.semaphore_wait(barrier, len(greeted))

    pair = (sp ^ 1, tp)
    swaps = [
        remote(give.at[0], kv.at[0, 0, mine], xs, xr, 0, pair),
        remote(give.at[1], kv.at[0, 1, mine], xs, xr, 1, pair),
        remote(give.at[2], qb.at[mine], xs, xr, 2, pair),
    ]
    for n, at in enumerate((0, 1)):
        local[at].wait()
        swaps[n].start()
    across, beside = (sp, tp ^ 2), (sp, tp ^ 1)
    half = owf.shape[1] // 2
    strip = half // pieces

    def strip_of(side, p):
        return pl.ds(pl.multiple_of(side * half + p * strip, strip), strip)

    def weight_copy(src, dst, side, p, slot, device):
        at = strip_of(side, p)
        return remote(owf.at[src, at], owf.at[dst, at], ws, wr, slot, device)

    near = remote(owf.at[0], owf.at[1], ws, wr, 4 * pieces, beside)
    wide = [weight_copy(0, 2, x, p, p, across) for p in range(pieces)]
    side = [weight_copy(2, 2, x, p, pieces + p, pair) for p in range(pieces)]
    pass_own = [weight_copy(2, 3, x, p, 2 * pieces + p, beside) for p in range(pieces)]
    pass_far = [weight_copy(2, 3, 1 - x, p, 3 * pieces + p, beside) for p in range(pieces)]
    twins = [
        remote(ids_ref.at[yy], ids_ref.at[yy], es, er, 0, across),
        remote(log_ref.at[yy], log_ref.at[yy], es, er, 1, across),
        remote(res_ref.at[yy], res_ref.at[yy], es, er, 2, across),
    ]

    def weight_step(p):
        wide[p].wait_recv()
        side[p].start()
        pass_own[p].start()

    def hop(d, part, h):
        where = mine if h == 0 else theirs
        slot = (d * 2 + part) * 2 + h
        return pltpu.make_async_remote_copy(
            src_ref=kv.at[d, part, where],
            dst_ref=kv.at[d + 1, part, where],
            send_sem=zs.at[slot],
            recv_sem=zr.at[slot],
            device_id=(sp + 2, tp),
            device_id_type=MESH,
        )

    log2e = 1.4426950408889634
    scale = hd ** (-0.5) * log2e
    k_tile = tri.shape[0]

    def block(d):
        offset = jnp.where(x == 0, off_ref[0], off_ref[1]) * log2e
        for kb in reversed(range(span // k_tile)):
            lead = kb * k_tile if d == 0 else 0
            at = pl.ds(lead, span - lead)
            query = qb[at, :]
            out, survive = acc[at, :], surv[at, :]
            keys = kv[d, 0, pl.ds(kb * k_tile, k_tile), :]
            scores = (
                lax.dot_general(
                    query, keys, (((1,), (1,)), ((), ())), preferred_element_type=f32
                )
                * scale
                - offset
            )
            drop = jnp.maximum(scores, 0.0) + log2e * jnp.log(1.0 + jnp.exp2(-jnp.abs(scores)))
            take = scores - drop
            if d == 0:
                causal = (
                    lax.broadcasted_iota(jnp.int32, scores.shape, 1)
                    < lax.broadcasted_iota(jnp.int32, scores.shape, 0)
                )
                drop = jnp.where(causal, drop, 0.0)
            top = drop.astype(bf16)
            low = (drop - top.astype(f32)).astype(bf16)
            tail = jnp.dot(top, tri[...], preferred_element_type=f32) + jnp.dot(
                low, tri[...], preferred_element_type=f32
            )
            weight = jnp.exp2(take + tail + survive)
            if d == 0:
                weight = jnp.where(causal, weight, 0.0)
            acc[at, :] = out + jnp.dot(
                weight.astype(bf16),
                kv[d, 1, pl.ds(kb * k_tile, k_tile), :],
                preferred_element_type=f32,
            )
            surv[at, :] = survive + (tail[:, :1] - drop[:, :1])

    local[2].wait()
    local[3].wait()

    @pl.when(has_next)
    def _():
        hop(0, 0, 0).start()
        hop(0, 1, 0).start()

    local[4].wait()
    swaps[2].start()
    local[7].wait()
    twins[0].start()
    local[8].wait()
    twins[1].start()
    local[5].wait()
    for copy in wide:
        copy.start()
    local[9].wait()
    twins[2].start()
    near.start()

    def receive(d, h):
        for part in range(2):
            hop(d - 1, part, h).wait_recv()
            if d + 1 < chain:

                @pl.when(has_next)
                def _():
                    hop(d, part, h).start()

    @pl.when(z >= 1)
    def _():
        receive(1, 0)

    swaps[0].wait_recv()
    swaps[1].wait_recv()

    @pl.when(has_next)
    def _():
        hop(0, 0, 1).start()
        hop(0, 1, 1).start()

    for at in (6, 10, 11, 12, 13, 14, 15):
        local[at].wait()
    swaps[2].wait_recv()
    weight_step(0)
    block(0)
    weight_step(1)
    for d in range(1, chain):

        @pl.when(d <= z)
        def _(d=d):
            if d > 1:
                receive(d, 0)
            receive(d, 1)
            block(d)

        if d == 1:
            for p in range(2, pieces):
                weight_step(p)
        if d == chain - 2:
            for p in range(pieces):
                side[p].wait_recv()
                pass_far[p].start()

    total = acc[...]
    normed = total * lax.rsqrt(jnp.mean(total * total, axis=1, keepdims=True) + head_eps)
    att[...] = (normed * hgain_ref[...]).astype(bf16).reshape(att.shape)

    def block_of(m):
        return att.at[x ^ (m & 1), :, core ^ ((m >> 1) & 1)]

    spread = [
        remote(block_of(m), th.at[m >> 1, x], ps, pr, m, device) for m, device in plane
    ]
    for copy in spread:
        copy.start()
    own = pltpu.make_async_copy(block_of(0), th.at[0, x], wsem.at[3])
    own.start()
    for copy in twins:
        copy.wait_recv()
    near.wait_recv()
    for copy in pass_own + pass_far:
        copy.wait_recv()
    own.wait()
    for copy in spread:
        copy.wait_recv()

    lefts = [
        jnp.concatenate([th[j, 0].reshape(-1, hd), th[j, 1].reshape(-1, hd)], axis=1)
        for j in range(4)
    ]
    col = min(512, width)
    for n in range(width // col):
        cut = pl.ds(n * col, col)
        mix[:, cut] = functools.reduce(
            jnp.add,
            [jnp.dot(lefts[j], owf[j, :, cut], preferred_element_type=f32) for j in range(4)],
        )
    hidden = layer_norm(
        residual_scale * res_ref[...].reshape(2 * row_count, width).astype(f32) + mix[...],
        g1_ref[...],
        b1_ref[...],
    ).astype(bf16)
    hid_ref[...] = hidden.reshape(2, row_count, width)
    chosen = [
        selection(ids_ref[yy], sp, capacity, experts),
        selection(ids_ref[1 - yy], sp, capacity, experts),
    ]
    pick = [functools.reduce(jnp.add, one).astype(bf16) for one in chosen]
    for n in range(width // col):
        cut = pl.ds(n * col, col)
        for r, many in ((0, experts), (1, dup)):
            picked = (
                jnp.dot(
                    pick[r][: many * capacity],
                    hid_ref[yy if r == 0 else 1 - yy, :, cut],
                    preferred_element_type=f32,
                )
                .astype(bf16)
                .reshape(many, capacity, col)
            )
            rows[0, 0, r, :, cut] = picked[0]
            out_ref[1:many, r, :, cut] = picked[1:]

    inner = jnp.logical_and(z > 0, has_next)
    flip = jnp.where(inner, 2, 0)

    def place(i):
        return i if i < half_dup else half_dup + ((i - half_dup) ^ (2 - flip))

    def partner(i):
        return (sp ^ i, tp)

    def send(i):
        if isinstance(i, int) and i < dup:
            return remote(out_ref.at[i], rows.at[i, 0], s0, r0, i, partner(i))
        return remote(out_ref.at[i, 0], rows.at[i, 0, 0], s0, r0, i, partner(i))

    def to_y(i):
        return remote(rows.at[i, 0, 0], rows.at[i, 0, 1], s1, r1, i, across)

    def to_core(i):
        if isinstance(i, int) and i < dup:
            return remote(rows.at[i, 0], rows.at[i, 1], s2, r2, i, beside)
        return remote(rows.at[i, 0, 0], rows.at[i, 1, 0], s2, r2, i, beside)

    def relay(i):
        return remote(rows.at[i, 0, 1], rows.at[i, 1, 1], s3, r3, i, beside)

    def swap_cores(i):
        return remote(part.at[i, 1], duo.at[i], s4, r4, i, beside)

    def sums(i):
        return remote(ysend.at[i - half_dup], yrecv.at[i - half_dup], s5, r5, i, across)

    def back(i):
        if isinstance(i, int) and i < half_dup:
            return remote(fin.at[i], ret.at[i], s6, r6, i, partner(i))
        return remote(fin_far.at[i - half_dup], ret_far.at[i - half_dup], s6, r6, i, partner(i))

    closing = [
        remote(csend.at[:, pl.ds(h * (width // 2), width // 2)],
               crecv.at[:, pl.ds(h * (width // 2), width // 2)], cs, cr, h, across)
        for h in range(2)
    ]
    def dispatch(i):
        send(i if i < half_dup else half_dup + ((i - half_dup) ^ (2 - flip))).start()

    tile, wide_col = min(256, units), min(512, width)
    gates_in, downs_in = units // tile, width // wide_col

    def enter(i):
        if i:
            send(place(i)).wait_recv()
        if i >= dup:
            to_y(place(i)).start()
        to_core(place(i)).start()

    def onward(i):
        if i >= dup:
            to_y(place(i)).wait_recv()
            relay(place(i)).start()

    def gather(g):
        for i in (2 * g, 2 * g + 1):
            to_core(place(i)).wait_recv()
            if i >= dup:
                relay(place(i)).wait_recv()

    def hidden_units(g, n):
        cut = pl.ds(n * tile, tile)
        given = rows[pl.ds(place(2 * g), 2)].reshape(-1, width)
        gate = jnp.dot(given, wg[:, cut], preferred_element_type=f32)
        up = jnp.dot(given, wu[:, cut], preferred_element_type=f32)
        act[:, cut] = (gate / (1.0 + jnp.exp(-gate)) * up).astype(bf16)

    def back_down(g, n):
        cut = pl.ds(n * wide_col, wide_col)
        down = jnp.dot(act[...], wd[:, cut], preferred_element_type=f32).astype(bf16)
        part[pl.ds(place(2 * g), 2), :, :, :, cut] = down.reshape(2, 2, 2, capacity, wide_col)

    def pair_up(i):
        swap_cores(place(i)).start()

    def cross(i):
        at = place(i)
        swap_cores(at).wait_recv()
        ysend[at - half_dup] = (part[at, 0, 1].astype(f32) + duo[at, 1].astype(f32)).astype(bf16)
        sums(at).start()

    def finish(i):
        at = place(i)
        if i >= half_dup:
            sums(at).wait_recv()
            fin_far[at - half_dup] = (
                part[at, 0, 0].astype(f32)
                + duo[at, 0].astype(f32)
                + yrecv[at - half_dup].astype(f32)
            ).astype(bf16)
        else:
            swap_cores(at).wait_recv()
            total = (part[at, 0].astype(f32) + duo[at].astype(f32)).astype(bf16)
            if i == 0:
                ret[0] = total
                return
            fin[i] = total
        back(at).start()

    def mixing_of(r, lead, many):
        logits = log_ref[yy if r == 0 else 1 - yy]
        high = jnp.max(logits, axis=0, keepdims=True)
        grown = jnp.exp(logits - high)
        gates = grown / jnp.sum(grown, axis=0, keepdims=True)
        mixing = functools.reduce(
            jnp.add,
            [
                one[lead * capacity : (lead + many) * capacity] * gates[k : k + 1, :]
                for k, one in enumerate(chosen[r])
            ],
        ).T
        top = mixing.astype(bf16)
        return top, (mixing - top.astype(f32)).astype(bf16)

    def mixed(parts, given):
        top, low = parts
        return jnp.dot(top, given, preferred_element_type=f32) + jnp.dot(
            low, given, preferred_element_type=f32
        )

    slots = half_dup * capacity

    def combine():
        ours, twin = mixing_of(0, 0, half_dup), mixing_of(1, 0, half_dup)
        for i in range(1, half_dup):
            back(i).wait_recv()
        for n in range(width // col):
            cut = pl.ds(n * col, col)
            csend[:, cut] = mixed(twin, ret[:, 1, :, cut].reshape(slots, col)).astype(bf16)
            mix[:row_count, cut] = mixed(ours, ret[:, 0, :, cut].reshape(slots, col))
        for copy in closing:
            copy.start()

    def close():
        for copy in closing:
            copy.wait_recv()
        mix[:row_count] = mix[:row_count] + crecv[...].astype(f32)

    def weights_in():
        for copy in weights:
            copy.wait()

    acts = {
        "F": enter, "R": onward, "G": gather, "P": pair_up, "X": cross, "N": finish,
        "U": hidden_units, "D": back_down, "W": weights_in, "S": dispatch, "K": combine, "L": close,
    }

    def run(token):
        acts[token[0]](*[int(v) for v in token[1:]])

    for number, token in enumerate(plan_of(gates_in, downs_in)):
        run(token)

    some = (experts - half_dup) // 2
    for lead in (half_dup + some, half_dup):
        far = mixing_of(0, lead, some)
        for i in range(lead, lead + some):
            back(i).wait_recv()
        at = lead - half_dup
        for n in range(width // col):
            cut = pl.ds(n * col, col)
            mix[:row_count, cut] = mix[:row_count, cut] + mixed(
                far, ret_far[at : at + some, :, cut].reshape(some * capacity, col)
            )
    y_ref[...] = layer_norm(
        residual_scale * hid_ref[yy].astype(f32) + mix[:row_count], g2_ref[...], b2_ref[...]
    ).astype(bf16)
    for copy in swaps + twins + wide + side + [near] + pass_own + pass_far + spread + closing:
        copy.wait_send()
    for i in range(experts):
        if i:
            send(i).wait_send()
            back(i).wait_send()
        to_core(i).wait_send()
        swap_cores(i).wait_send()
        if i >= dup:
            to_y(i).wait_send()
            relay(i).wait_send()
        if i >= half_dup:
            sums(i).wait_send()
    for d in range(chain - 1):

        @pl.when(jnp.logical_and(d <= z, has_next))
        def _(d=d):
            for h in range(2):
                for part_of in range(2):
                    hop(d, part_of, h).wait_send()


def fused(
    queries, keys, values, score_offset, head_gain, out_weight, residual, ln1_gain, ln1_bias,
    expert_ids, route_logits, gate_weight, up_weight, down_weight, ln2_gain, ln2_bias,
):
    experts = lax.axis_size("sp")
    tok, hd = queries.shape[0], head_gain.shape[0]
    row_count, width = residual.shape
    top_count = expert_ids.shape[1]
    capacity = max(2, 2 * top_count * row_count // experts)
    chain = experts // 2
    span = 2 * tok
    pieces, dup = 4, 2
    units = gate_weight.shape[2]
    hbm = pl.BlockSpec(memory_space=pl.ANY)
    dma = lambda n: pltpu.SemaphoreType.DMA((n,))
    limit = 56 * 1024 * 1024
    block = lambda *lead: pltpu.VMEM((*lead, capacity, width), bf16)
    line = lambda n: pltpu.VMEM((1, n), f32)
    n = experts
    return pl.pallas_call(
        functools.partial(layer_kernel, chain, experts, capacity, pieces, dup),
        out_shape=pltpu.VMEM((row_count, width), bf16),
        in_specs=[hbm] * 16,
        out_specs=pl.BlockSpec(memory_space=pltpu.VMEM),
        scratch_shapes=[
            pltpu.SMEM(score_offset.shape, f32),
            line(hd), line(width), line(width), line(width), line(width),
            pltpu.VMEM((2, top_count, row_count), jnp.int32),
            pltpu.VMEM((2, top_count, row_count), f32),
            pltpu.VMEM((2, row_count, width), bf16),
            pltpu.VMEM((3, tok, hd), bf16),
            pltpu.VMEM((2, row_count, width), bf16),
            block(n, 2),
            pltpu.VMEM((chain, 2, span, hd), bf16),
            pltpu.VMEM((span, hd), bf16),
            pltpu.VMEM((span, hd), f32),
            pltpu.VMEM((span, 1), f32),
            pltpu.VMEM((min(256, tok), min(256, tok)), bf16),
            pltpu.VMEM((2, 2, 2, row_count, hd), bf16),
            pltpu.VMEM((4, 2, 2, row_count, hd), bf16),
            pltpu.VMEM((4, out_weight.shape[0], width), bf16),
            pltpu.VMEM((2 * row_count, width), f32),
            block(n, 2, 2),
            pltpu.VMEM((width, units), bf16),
            pltpu.VMEM((width, units), bf16),
            pltpu.VMEM((units, width), bf16),
            pltpu.VMEM((8 * capacity, units), bf16),
            block(n, 2, 2), block(n, 2), block(n // 2), block(n // 2),
            block(n // 2, 2), block(n // 2), block(n // 2, 2), block(n // 2),
            pltpu.VMEM((row_count, width), bf16), pltpu.VMEM((row_count, width), bf16),
            dma(16), dma(3), dma(3), dma(4 * chain), dma(4 * chain), dma(8), dma(8),
            dma(4 * pieces + 1), dma(4 * pieces + 1),
            dma(4),
            dma(n), dma(n), dma(n), dma(n), dma(n), dma(n), dma(n), dma(n),
            dma(n), dma(n), dma(n), dma(n), dma(n), dma(n), dma(3), dma(3), dma(2), dma(2),
        ],
        compiler_params=pltpu.CompilerParams(
            collective_id=0, has_side_effects=True, vmem_limit_bytes=limit
        ),
    )(
        queries, keys, values, score_offset, head_gain[None], out_weight, residual,
        ln1_gain[None], ln1_bias[None], expert_ids.T, route_logits.T,
        ln2_gain[None], ln2_bias[None], gate_weight, up_weight, down_weight,
    )


def program_for(*args):
    queries, head_gain, residual, ids = args[0], args[4], args[6], args[9]
    experts = lax.axis_size("sp")
    capacity = max(2, 2 * ids.shape[1] * residual.shape[0] // experts)
    rows_ok = capacity % 16 == 0 and residual.shape[0] % 16 == 0
    heads_ok = queries.shape[1] == 2 * head_gain.shape[0] and head_gain.shape[0] % 128 == 0
    mesh_ok = lax.axis_size("tp") == 4 and experts == 8
    whole = queries.shape[0] % 128 == 0 and args[11].shape[0] == 1
    if rows_ok and heads_ok and mesh_ok and whole:
        return fused(*args)
    return on_device(*args)


def solution(mesh):
    in_specs = (
        P("sp", "tp"),
        P("sp", "tp"),
        P("sp", "tp"),
        P("tp"),
        P(),
        P("tp", None),
        P(("sp", "tp"), None),
        P(),
        P(),
        P(("sp", "tp"), None),
        P(("sp", "tp"), None),
        P("sp", None, "tp"),
        P("sp", None, "tp"),
        P("sp", "tp", None),
        P(),
        P(),
    )
    out_specs = P(("sp", "tp"), None)
    return jax.shard_map(
        program_for, mesh=mesh, in_specs=in_specs, out_specs=out_specs, check_vma=False
    )
```
